256 devices in a mesh: ep: 128 (over z, y, x), tp: 2 (over core).
Axes of the slice: x: 4, y: 4, z: 8, core: 2. Of those that a mesh axis runs over, the one named last changes fastest.
Arguments:
- tokens: bfloat16 [4096, 2048], P('ep'), may hold values from -6 to 6
- mix_gain: float32 [2048], replicated, may hold values from 0.1 to 1.9
- w_query: bfloat16 [2048, 512], P('ep', 'tp'), may hold values from -0.125 to 0.125
- w_key: bfloat16 [2048, 512], P('ep', 'tp'), may hold values from -0.125 to 0.125
- w_value: bfloat16 [2048, 512], P('ep', 'tp'), may hold values from -0.125 to 0.125
- w_outgate: bfloat16 [2048, 512], P('ep', 'tp'), may hold values from -0.125 to 0.125
- w_igate: bfloat16 [2048, 8], P('ep', 'tp'), may hold values from -0.125 to 0.125
- w_fgate: bfloat16 [2048, 8], P('ep', 'tp'), may hold values from -0.125 to 0.125
- igate_bias: float32 [8], P('tp'), may hold values from -2 to 1
- fgate_bias: float32 [8], P('tp'), may hold values from 0 to 4
- head_gain: float32 [512], P('tp'), may hold values from 0.1 to 1.9
- w_out: bfloat16 [512, 2048], P('tp', 'ep'), may hold values from -0.25 to 0.25
- state_matrix: float32 [4096, 8, 64, 64], P('ep', 'tp'), may hold values from -2.4 to 2.4
- state_norm: float32 [4096, 8, 64], P('ep', 'tp'), may hold values from -2.4 to 2.4
- state_max: float32 [4096, 8], P('ep', 'tp'), may hold values from -4 to 4
- ffn_gain: float32 [2048], replicated, may hold values from 0.1 to 1.9
- w_expert_gate: bfloat16 [128, 2048, 1408], P('ep', None, 'tp'), may hold values from -0.125 to 0.125
- w_expert_up: bfloat16 [128, 2048, 1408], P('ep', None, 'tp'), may hold values from -0.125 to 0.125
- w_expert_down: bfloat16 [128, 1408, 2048], P('ep', 'tp'), may hold values from -0.15625 to 0.15625
- routes: int32 [4096, 3], P('ep'), may hold values from 0 to 127, all different within a row; in each aligned block of 32 rows (0 to 31, 32 to 63, ...) at most 2 rows name the same one
- route_weights: float32 [4096, 3], P('ep'), may hold values from 0.2 to 1
Outputs:
- mixed: bfloat16 [4096, 2048], P('ep')
- new_matrix: float32 [4096, 8, 64, 64], P('ep', 'tp')
- new_norm: float32 [4096, 8, 64], P('ep', 'tp')
- new_max: float32 [4096, 8], P('ep', 'tp')
The draws below stay inside these ranges and needn't reach their ends.
Inputs may be any that keep to these rules, and one draw needn't show every extreme that they name: `routes`: each row names 3 different experts. Among the rows of one device, no expert is named by more than 2 rows, a bound that some block reaches.
All inputs are finite; a program needn't handle non-finite values.
Results may differ from the reference program's by a relative error of at most 0.017.
Values may be sent and summed in bfloat16 or wider, within the bound.
A program may use at most 128 MiB of HBM per device.

```python
import math
import jax
import jax.numpy as jnp
import numpy as np
from jax import lax

D = 2048
HEADS = 8
HEAD_SIZE = 64
HW = 512
D_EXP = 1408
TOPK = 3
EXPERTS = 128
SEQ_DEV = 32
B = 4096
CAP = 2
N_EP = 128
N_TP = 2


def steps_of(stream_key, shape, split, low, high):
    level = 1.0
    for position, shards_of in split:
        draws = jax.random.uniform(jax.random.fold_in(jax.random.fold_in(stream_key, 6), position), (shards_of,), jnp.float32, low / len(split), high / len(split))
        level = level * jnp.repeat(jnp.exp(draws), shape[position] // shards_of).reshape((-1,) + (1,) * (len(shape) - 1 - position))
    return level


def routed_block(stream_key, own, number, rows, amount, top, reach, lean):
    order = jax.random.permutation(stream_key, amount)
    packed, usual = load_shares(amount, rows * top, reach, lean, True), load_shares(amount, rows * top, reach, lean, False)
    places = jnp.arange(amount)

    def named(tallies, offset_by):
        used = int((tallies > 0).sum())
        fixed = max(1, used // 4)
        shifted = fixed + (places - fixed + offset_by * (used - fixed)) % max(1, amount - fixed)
        return jnp.zeros((amount,), jnp.int32).at[order[jnp.where(places < fixed, places, shifted)]].set(jnp.asarray(tallies, jnp.int32))

    tallies = jnp.where(number % 4 == 0, named(packed, number // 4), named(usual, number - number // 4 - 1))
    mixed = jax.random.permutation(jax.random.fold_in(own, 3), amount)
    source_of, sink = mixed[0:amount // 2 * 2:2], mixed[1:amount // 2 * 2:2]
    room = jnp.minimum(tallies[source_of] - 1, reach - tallies[sink]) // 2
    room = jnp.where((source_of == order[0]) | (sink == order[0]) | (tallies[sink] == 0), 0, jnp.maximum(room, 0))
    shifted = jax.random.randint(jax.random.fold_in(own, 4), (amount // 2,), 0, 1 << 20) % (room + 1)
    tallies = tallies.at[source_of].add(-shifted).at[sink].add(shifted)
    labels = jnp.searchsorted(jnp.cumsum(tallies), jnp.arange(rows * top), side="right").astype(jnp.int32)
    listing = labels.reshape(top, rows).T
    listing = listing[jax.random.permutation(jax.random.fold_in(own, 1), rows)]
    offset_by = jax.random.randint(jax.random.fold_in(own, 2), (rows, 1), 0, top)
    return jnp.take_along_axis(listing, (jnp.arange(top)[None, :] + offset_by) % top, axis=1)


def load_shares(number_of, total, reach, lean, full):
    loads = [(1 << 20) // math.isqrt(rank ** lean) + 1 for rank in range(1, number_of + 1)]
    largest = reach if full else min(reach, max(-(-total // number_of), total * loads[0] // sum(loads)))
    least = 1 if total - largest >= number_of - 1 else 0
    given, rest = [largest] + [least] * (number_of - 1), total - largest - least * (number_of - 1)
    while rest > 0:
        candidates = [i for i in range(1, number_of) if given[i] < largest] or [i for i in range(1, number_of) if given[i] < reach]
        pool, budget = sum([loads[i] for i in candidates]), rest
        for i in candidates:
            more = min(reach - given[i], max(1, budget * loads[i] // pool), rest)
            given[i] = given[i] + more
            rest = rest - more
    return np.array(given)


def normal_values(key, dims, spread, limit, pieces=(), kind=jnp.bfloat16):
    values = jax.random.normal(key, dims, jnp.float32) * spread
    if len(pieces) > 0:
        values = steps_of(key, dims, pieces, -0.22, 0.18) * values
    return jnp.clip(values, min=-limit, max=limit).astype(kind)


def setup_inputs(seed: int = 0) -> dict:
    arg_keys = jax.random.split(jax.random.key(seed), 22)
    tokens = normal_values(arg_keys[0], (B, D), 1.0, 6.0, ((0, 128),))
    mix_gain = jnp.clip(1.0 + 0.18 * jax.random.normal(arg_keys[1], (D,), jnp.float32), 0.1, 1.9)
    w_query = normal_values(arg_keys[2], (D, HW), D ** -0.5, 0.125, ((0, 128), (1, 2)))
    w_key = normal_values(arg_keys[3], (D, HW), D ** -0.5, 0.125, ((0, 128), (1, 2)))
    w_value = normal_values(arg_keys[4], (D, HW), D ** -0.5, 0.125, ((0, 128), (1, 2)))
    w_outgate = normal_values(arg_keys[5], (D, HW), D ** -0.5, 0.125, ((0, 128), (1, 2)))
    w_igate = normal_values(arg_keys[6], (D, HEADS), D ** -0.5, 0.125, ((0, 128), (1, 2)))
    w_fgate = normal_values(arg_keys[7], (D, HEADS), D ** -0.5, 0.125, ((0, 128), (1, 2)))
    igate_bias = jnp.clip(-2.0 + 3.0 * jax.random.uniform(arg_keys[8], (HEADS,), jnp.float32) ** steps_of(arg_keys[8], (HEADS,), ((0, 2),), -0.2, 0.2), -2.0, 1.0)
    fgate_bias = jnp.clip(4.0 * jax.random.uniform(arg_keys[9], (HEADS,), jnp.float32) ** steps_of(arg_keys[9], (HEADS,), ((0, 2),), -0.2, 0.2), 0.0, 4.0)
    head_gain = jnp.clip(1.0 + 0.18 * jax.random.normal(arg_keys[10], (HW,), jnp.float32), 0.1, 1.9)
    w_out = normal_values(arg_keys[11], (HW, D), HW ** -0.5, 0.25, ((0, 2), (1, 128)))
    state_matrix = normal_values(arg_keys[12], (B, HEADS, HEAD_SIZE, HEAD_SIZE), 0.3, 2.4, ((0, 128), (1, 2)), jnp.float32)
    state_norm = normal_values(arg_keys[13], (B, HEADS, HEAD_SIZE), 0.3, 2.4, ((0, 128), (1, 2)), jnp.float32)
    state_max = normal_values(arg_keys[14], (B, HEADS), 1.0, 4.0, ((0, 128), (1, 2)), jnp.float32)
    ffn_gain = jnp.clip(1.0 + 0.18 * jax.random.normal(arg_keys[15], (D,), jnp.float32), 0.1, 1.9)
    w_expert_gate = normal_values(arg_keys[16], (EXPERTS, D, D_EXP), D ** -0.5, 0.125, ((0, 128), (2, 2)))
    w_expert_up = normal_values(arg_keys[17], (EXPERTS, D, D_EXP), D ** -0.5, 0.125, ((0, 128), (2, 2)))
    w_expert_down = normal_values(arg_keys[18], (EXPERTS, D_EXP, D), D_EXP ** -0.5, 0.15625, ((0, 128), (1, 2)))
    routes_keys = jax.random.split(jax.random.fold_in(arg_keys[19], 1), B // SEQ_DEV)
    routes_turns = jax.random.permutation(jax.random.fold_in(arg_keys[19], 3), B // SEQ_DEV)
    routes = jax.vmap(lambda own, number: routed_block(jax.random.fold_in(arg_keys[19], 2), own, number, SEQ_DEV, EXPERTS, TOPK, CAP, 2))(routes_keys, routes_turns).reshape((B, TOPK))
    route_weights = jnp.clip(0.2 + 0.8 * jax.random.uniform(arg_keys[20], (B, TOPK), jnp.float32) ** steps_of(arg_keys[20], (B, TOPK), ((0, 128),), -0.2, 0.2), 0.2, 1.0)
    return {"tokens": tokens, "mix_gain": mix_gain, "w_query": w_query, "w_key": w_key, "w_value": w_value, "w_outgate": w_outgate, "w_igate": w_igate, "w_fgate": w_fgate, "igate_bias": igate_bias, "fgate_bias": fgate_bias, "head_gain": head_gain, "w_out": w_out, "state_matrix": state_matrix, "state_norm": state_norm, "state_max": state_max, "ffn_gain": ffn_gain, "w_expert_gate": w_expert_gate, "w_expert_up": w_expert_up, "w_expert_down": w_expert_down, "routes": routes, "route_weights": route_weights}


def rms_scale(values_in, gain_vec):
    widened = values_in.astype(jnp.float32)
    return widened * lax.rsqrt(lax.optimization_barrier(jnp.mean(widened * widened, axis=-1, keepdims=True)) + 1e-06) * gain_vec

def memory_cell(query, key_row, value_row, outgate, input_pre, forget_pre, head_gain, state_matrix, state_norm, state_max):
    seq_rows, head_count = input_pre.shape
    head_size = query.shape[1] // head_count
    query_heads = query.astype(jnp.float32).reshape(seq_rows, head_count, head_size)
    key_heads = key_row.astype(jnp.float32).reshape(seq_rows, head_count, head_size) * head_size ** (-0.5)
    value_heads = value_row.astype(jnp.float32).reshape(seq_rows, head_count, head_size)
    log_forget = jax.nn.log_sigmoid(forget_pre)
    new_max = jnp.maximum(log_forget + state_max, input_pre)
    keep_old = jnp.exp(log_forget + state_max - new_max)
    keep_new = jnp.exp(input_pre - new_max)
    new_matrix = keep_old[:, :, None, None] * state_matrix + keep_new[:, :, None, None] * value_heads[:, :, :, None] * key_heads[:, :, None, :]
    new_norm = keep_old[:, :, None] * state_norm + keep_new[:, :, None] * key_heads
    numerator = jnp.einsum('bhvd,bhd->bhv', new_matrix, query_heads, precision=lax.Precision.HIGHEST)
    denominator = lax.optimization_barrier(jnp.sum(new_norm * query_heads, axis=-1))
    cell_read = numerator / jnp.maximum(jnp.abs(denominator), jnp.exp(-new_max))[:, :, None]
    centered = cell_read - lax.optimization_barrier(jnp.mean(cell_read, axis=-1, keepdims=True))
    variance = lax.optimization_barrier(jnp.mean(centered * centered, axis=-1, keepdims=True))
    scaled_cell = (centered * lax.rsqrt(variance + 1e-06)).reshape(seq_rows, head_count * head_size)
    cell_out = (scaled_cell * head_gain * jax.nn.sigmoid(outgate.astype(jnp.float32))).astype(jnp.bfloat16)
    return (cell_out, new_matrix, new_norm, new_max)

def reference(tokens, mix_gain, w_query, w_key, w_value, w_outgate, w_igate, w_fgate, igate_bias, fgate_bias, head_gain, w_out, state_matrix, state_norm, state_max, ffn_gain, w_expert_gate, w_expert_up, w_expert_down, routes, route_weights):
    normed = rms_scale(tokens, mix_gain).astype(jnp.bfloat16)

    def project(weight):
        return jnp.dot(normed, weight, preferred_element_type=jnp.float32)
    query = project(w_query).astype(jnp.bfloat16)
    key_row = project(w_key).astype(jnp.bfloat16)
    value_row = project(w_value).astype(jnp.bfloat16)
    outgate = project(w_outgate).astype(jnp.bfloat16)
    input_pre = project(w_igate) + igate_bias
    forget_pre = project(w_fgate) + fgate_bias
    cell_out, new_matrix, new_norm, new_max = memory_cell(query, key_row, value_row, outgate, input_pre, forget_pre, head_gain, state_matrix, state_norm, state_max)
    seq_rows, width = tokens.shape
    cell_width = cell_out.shape[1]
    blocks = jnp.einsum('bth,thd->btd', cell_out.astype(jnp.float32).reshape(seq_rows, N_TP, cell_width // N_TP), w_out.astype(jnp.float32).reshape(N_TP, cell_width // N_TP, width))
    rounded = lax.optimization_barrier(blocks.astype(jnp.bfloat16))
    resid = (tokens.astype(jnp.float32) + lax.optimization_barrier(jnp.sum(rounded.astype(jnp.float32), axis=1))).astype(jnp.bfloat16)
    normed_two = rms_scale(resid, ffn_gain).astype(jnp.bfloat16)
    groups = N_EP
    per_group = seq_rows // groups
    expert_total = w_expert_gate.shape[0]
    top_count = routes.shape[1]
    flat_routes = routes.reshape(groups, per_group * top_count)
    onehot = (flat_routes[:, :, None] == jnp.arange(expert_total, dtype=jnp.int32)[None, None, :]).astype(jnp.int32)
    earlier = jnp.cumsum(onehot, axis=1, dtype=jnp.int32) - onehot
    slots = lax.optimization_barrier(jnp.sum(onehot * earlier, axis=-1, dtype=jnp.int32)).astype(jnp.int32)
    group_ids = jnp.broadcast_to(jnp.arange(groups, dtype=jnp.int32)[:, None], flat_routes.shape)
    token_ids = (jnp.arange(seq_rows * top_count, dtype=jnp.int32) // top_count).reshape(groups, per_group * top_count)
    table = jnp.zeros((expert_total, groups, CAP), jnp.int32).at[flat_routes, group_ids, slots].set(token_ids)

    def run_expert(operands):
        gate_weight, up_weight, down_weight, row_ids = operands
        rows = normed_two[row_ids.reshape(-1)]
        gate_pre = jnp.dot(rows, gate_weight, preferred_element_type=jnp.float32)
        up_pre = jnp.dot(rows, up_weight, preferred_element_type=jnp.float32)
        hidden = (jax.nn.silu(gate_pre) * up_pre).astype(jnp.bfloat16)
        expert_width = hidden.shape[1]
        parts = jnp.einsum('rtf,tfd->rtd', hidden.astype(jnp.float32).reshape(-1, N_TP, expert_width // N_TP), down_weight.astype(jnp.float32).reshape(N_TP, expert_width // N_TP, width))
        rounded_parts = lax.optimization_barrier(parts.astype(jnp.bfloat16))
        return lax.optimization_barrier(jnp.sum(rounded_parts.astype(jnp.float32), axis=1)).astype(jnp.bfloat16)
    outputs = lax.map(run_expert, (w_expert_gate, w_expert_up, w_expert_down, table))
    picked = outputs[flat_routes, group_ids * CAP + slots]
    picked = picked.reshape(seq_rows, top_count, width).astype(jnp.float32)
    mixed = (resid.astype(jnp.float32) + lax.optimization_barrier(jnp.sum(picked * route_weights[:, :, None], axis=1))).astype(jnp.bfloat16)
    return (mixed, new_matrix, new_norm, new_max)
```

```python
import jax
import jax.numpy as jnp
from jax import lax
from jax.experimental import pallas as pl
from jax.experimental.pallas import tpu as pltpu
from jax.sharding import Mesh
from jax.sharding import PartitionSpec as P

EP = ("ep_0", "ep_1", "ep_2")
NZ, NY, NX = 8, 4, 4
NP = NY * NX
D, HALF = 2048, 1024
DE = 704
ROWS = 32
MESH = pl.DeviceIdType.MESH
F32, BF16 = jnp.float32, jnp.bfloat16


def whereami():
    return (
        lax.axis_index("ep_0"),
        lax.axis_index("ep_1"),
        lax.axis_index("ep_2"),
        lax.axis_index("tp"),
    )


def push(src, dst, send_sem, recv_sem, to):
    return pltpu.make_async_remote_copy(
        src_ref=src,
        dst_ref=dst,
        send_sem=send_sem,
        recv_sem=recv_sem,
        device_id=to,
        device_id_type=MESH,
    )


def nt_dot(a, b):
    return lax.dot_general(a, b, (((1,), (1,)), ((), ())), preferred_element_type=F32)


def nn_dot(a, b):
    return jnp.dot(a, b, preferred_element_type=F32)


def rms_scale(values, gain):
    return values * lax.rsqrt(jnp.mean(values * values, axis=-1, keepdims=True) + 1e-06) * gain


def gather_kernel(
    tok_ref, gain_ref, wp_ref, wo_ref,
    proj_ref, gates_ref, wof_ref,
    nall, wst, gsum, wfull, gt, woz, res,
    n_s, n_r, f_s, f_r, w_s, w_r, o_s, o_r, x_s, x_r, g_s, g_r, v_s, v_r, p_s, p_r,
):
    z, y, x, c = whereami()
    yx = y * NX + x
    half = pl.ds(pl.multiple_of(c * HALF, HALF), HALF)
    other = pl.ds(pl.multiple_of((1 - c) * HALF, HALF), HALF)
    partner = (z, y, x, 1 - c)

    def zpeer(d):
        return (z + d) % NZ

    def ppeer(d):
        yt, xt = (y + d // NX) % NY, (x + d % NX) % NX
        return yt, xt, yt * NX + xt

    barrier = pltpu.get_barrier_semaphore()
    for d in range(1, NZ):
        pl.semaphore_signal(barrier, 1, device_id=(zpeer(d), y, x, c), device_id_type=MESH)

    def greet(d, carry):
        yt, xt, _ = ppeer(d)
        pl.semaphore_signal(barrier, 1, device_id=(z, yt, xt, c), device_id_type=MESH)
        return carry

    lax.fori_loop(1, NP, greet, 0)
    pl.semaphore_signal(barrier, 1, device_id=partner, device_id_type=MESH)

    nall[z] = rms_scale(tok_ref[...].astype(F32), gain_ref[...]).astype(BF16)
    wst[z] = wp_ref[z]
    woz[z] = wo_ref[...]

    pl.semaphore_wait(barrier, NZ - 1 + NP - 1 + 1)

    order = (4, 3, 5, 2, 6, 1, 7)

    def w_send(d):
        zt = zpeer(d)
        return push(wp_ref.at[zt], wst.at[z], w_s.at[zt], w_r.at[z], (zt, y, x, c))

    def o_send(d):
        zt = zpeer(d)
        return push(wo_ref, woz.at[z], o_s.at[zt], o_r.at[z], (zt, y, x, c))

    def n_send(d):
        zt = zpeer(d)
        return push(nall.at[z, :, half], nall.at[z, :, half], n_s.at[zt], n_r.at[z], (zt, y, x, c))

    for d in order:
        w_send(d).start()
    for d in order:
        o_send(d).start()
    for d in order:
        n_send(d).start()

    def arrived(src, dst, recv_sem):
        push(src, dst, recv_sem, recv_sem, partner).wait_recv()

    for d in range(1, NZ):
        zs = zpeer(d)
        arrived(wst.at[zs], wst.at[zs], w_r.at[zs])
    total = wst[0, 16:32, :].astype(F32)
    for k in range(1, NZ):
        total = total + wst[k, 16:32, :].astype(F32)
    gsum[...] = total.astype(BF16)
    gt[yx] = gsum[...]
    for k in range(NZ):
        wfull[k, yx] = wst[k, 0:16, :]

    def x_send(d):
        yt, xt, yxt = ppeer(d)
        return push(wst.at[:, 0:16, :], wfull.at[:, yx], x_s.at[yxt], x_r.at[yx], (z, yt, xt, c))

    def g_send(d):
        yt, xt, yxt = ppeer(d)
        return push(gsum, gt.at[yx], g_s.at[yxt], g_r.at[yx], (z, yt, xt, c))

    def v_send(d):
        yt, xt, yxt = ppeer(d)
        return push(woz, wof_ref.at[:, yx], v_s.at[yxt], v_r.at[yx], (z, yt, xt, c))

    def start_xg(d, carry):
        x_send(d).start()
        g_send(d).start()
        return carry

    lax.fori_loop(1, NP, start_xg, 0)

    for d in range(1, NZ):
        zs = zpeer(d)
        arrived(woz.at[zs], woz.at[zs], o_r.at[zs])
    for k in range(NZ):
        wof_ref[k, yx] = woz[k]

    def start_v(d, carry):
        v_send(d).start()
        return carry

    lax.fori_loop(1, NP, start_v, 0)

    def f_send(zs):
        return push(nall.at[zs, :, half], nall.at[zs, :, half], f_s.at[zs], f_r.at[zs], partner)

    for d in (1, 7, 2, 6, 3, 5, 4):
        zs = zpeer(d)
        arrived(nall.at[zs, :, half], nall.at[zs, :, half], n_r.at[zs])
        f_send(zs).start()
    for d in (1, 7, 2, 6, 3, 5, 4):
        zs = zpeer(d)
        arrived(nall.at[zs, :, other], nall.at[zs, :, other], f_r.at[zs])

    def wait_xg(d, carry):
        _, _, s = ppeer(d)
        arrived(wfull.at[:, s], wfull.at[:, s], x_r.at[s])
        arrived(gt.at[s], gt.at[s], g_r.at[s])
        return carry

    lax.fori_loop(1, NP, wait_xg, 0)

    every = nn_dot(nall[...].reshape(NZ * ROWS, D), wfull[...].reshape(D, 128))
    res[...] = every.astype(BF16).reshape(NZ, ROWS, 128)
    proj_ref[z] = res[z]

    def p_send(d):
        zt = zpeer(d)
        return push(res.at[zt], proj_ref.at[z], p_s.at[zt], p_r.at[z], (zt, y, x, c))

    for d in order:
        p_send(d).start()

    mine = nall[z]
    stacked = jnp.concatenate([mine[:, 256 * k:256 * (k + 1)] for k in range(NZ)], axis=0)
    gp = nn_dot(stacked, gt[...].reshape(256, 128))
    group = lax.broadcasted_iota(jnp.int32, (ROWS, 128), 1) // 8
    acc = jnp.zeros((ROWS, 128), F32)
    for k in range(NZ):
        acc = acc + jnp.where(group == k, gp[ROWS * k:ROWS * (k + 1)], 0.0)
    for shift in (64, 32, 16, 8):
        acc = acc + pltpu.roll(acc, shift, 1)
    gates_ref[...] = acc

    for d in range(1, NZ):
        zs = zpeer(d)
        arrived(proj_ref.at[zs], proj_ref.at[zs], p_r.at[zs])

    def wait_v(d, carry):
        _, _, s = ppeer(d)
        arrived(wof_ref.at[:, s], wof_ref.at[:, s], v_r.at[s])
        return carry

    lax.fori_loop(1, NP, wait_v, 0)

    for d in range(1, NZ):
        w_send(d).wait_send()
        o_send(d).wait_send()
        n_send(d).wait_send()
        f_send(zpeer(d)).wait_send()
        p_send(d).wait_send()

    def sent(d, carry):
        x_send(d).wait_send()
        g_send(d).wait_send()
        v_send(d).wait_send()
        return carry

    lax.fori_loop(1, NP, sent, 0)


def gather(tokens, mix_gain, wp, wo_t):
    dma = pltpu.SemaphoreType.DMA
    vm = pl.BlockSpec(memory_space=pltpu.VMEM)
    sems = []
    for count in (NZ, NZ, NZ, NZ, NP, NP, NP, NZ):
        sems += [dma((count,)), dma((count,))]
    return pl.pallas_call(
        gather_kernel,
        name="gather",
        out_shape=(
            jax.ShapeDtypeStruct((NZ, ROWS, 128), BF16),
            jax.ShapeDtypeStruct((ROWS, 128), F32),
            jax.ShapeDtypeStruct((NZ, NP, 16, 256), BF16),
        ),
        in_specs=[vm] * 4,
        out_specs=(vm, vm, vm),
        scratch_shapes=[
            pltpu.VMEM((NZ, ROWS, D), BF16),
            pltpu.VMEM((NZ, 32, 128), BF16),
            pltpu.VMEM((16, 128), BF16),
            pltpu.VMEM((NZ, NP, 16, 128), BF16),
            pltpu.VMEM((NP, 16, 128), BF16),
            pltpu.VMEM((NZ, 16, 256), BF16),
            pltpu.VMEM((NZ, ROWS, 128), BF16),
            *sems,
        ],
        compiler_params=pltpu.CompilerParams(
            collective_id=0, has_side_effects=True, vmem_limit_bytes=32 << 20
        ),
    )(tokens, mix_gain.reshape(1, D), wp, wo_t)


def expert_kernel(
    cell_ref, tok_ref, gain_ref, wof_ref, crow_ref, ccol_ref, wcol_ref, wg_hbm, wu_hbm, wd_hbm,
    mixed_ref,
    p_my, p_ot, resid, ntwo, amat, whi, wlo, outt, rcv, xf, xm, wg, wu, wd, hid, pd, pd_ot, back, ret,
    ld, q_s, q_r, d_s, d_r, h_s, h_r, k_s, k_r, b_s, b_r, m_s, m_r,
):
    z, y, x, c = whereami()
    yx = y * NX + x
    me = z * NP + yx
    partner = (z, y, x, 1 - c)
    half = pl.ds(pl.multiple_of(c * HALF, HALF), HALF)
    other = pl.ds(pl.multiple_of((1 - c) * HALF, HALF), HALF)

    loads = [
        pltpu.make_async_copy(wg_hbm.at[0], wg, ld.at[0]),
        pltpu.make_async_copy(wu_hbm.at[0], wu, ld.at[1]),
        pltpu.make_async_copy(wd_hbm.at[0], wd, ld.at[2]),
    ]
    for load in loads:
        load.start()

    def place(i, j):
        zt = (z + i) % NZ
        yt, xt = (y + j // NX) % NY, (x + j % NX) % NX
        return (zt, yt, xt, c), zt * NP + yt * NX + xt

    def over_peers(body):
        def outer(i, carry):
            def inner(j, carry2):
                body(i, j)
                return carry2

            lax.fori_loop(jnp.where(i == 0, 1, 0), NP, inner, 0)
            return carry

        lax.fori_loop(0, NZ, outer, 0)

    barrier = pltpu.get_barrier_semaphore()

    def greet(i, j):
        to, _ = place(i, j)
        pl.semaphore_signal(barrier, 1, device_id=to, device_id_type=MESH)

    over_peers(greet)
    pl.semaphore_signal(barrier, 1, device_id=partner, device_id_type=MESH)

    part = nt_dot(cell_ref[...], wof_ref[...].reshape(D, 256))
    p_my[...] = part.astype(BF16)

    def build_a(i, carry):
        at = pl.ds(pl.multiple_of(i * 256, 256), 256)
        row = lax.broadcasted_iota(jnp.int32, (256, 256), 0) + i * 256
        hit = (row == crow_ref[0:1, :]) | (row == crow_ref[1:2, :]) | (row == crow_ref[2:3, :])
        amat[at, :] = jnp.where(hit, 1.0, 0.0).astype(BF16)
        col = lax.broadcasted_iota(jnp.int32, (256, 256), 1) + i * 256
        weight = jnp.zeros((256, 256), F32)
        for k in range(3):
            weight = weight + jnp.where(col == ccol_ref[:, k:k + 1], wcol_ref[:, k:k + 1], 0.0)
        high = weight.astype(BF16)
        whi[:, at] = high
        wlo[:, at] = (weight - high.astype(F32)).astype(BF16)
        return carry

    lax.fori_loop(0, 8, build_a, 0)

    pl.semaphore_wait(barrier, NZ * NP)

    swap = push(p_my, p_ot, q_s, q_r, partner)
    swap.start()
    swap.wait_recv()
    total = p_my[...].astype(F32) + p_ot[...].astype(F32)
    res = (tok_ref[...].astype(F32) + total).astype(BF16)
    resid[...] = res
    ntwo[...] = rms_scale(res.astype(F32), gain_ref[...]).astype(BF16)

    def cols(k):
        return pl.ds(pl.multiple_of(c * HALF + k * 128, 128), 128)

    xr = jnp.concatenate([ntwo[:, cols(k)] for k in range(8)], axis=0)

    def d_send(i, j):
        to, e = place(i, j)
        return push(outt.at[e], rcv.at[c, me], d_s.at[e], d_r.at[me], to)

    def dispatch(i, carry):
        zt = (z + i) % NZ
        rows = nn_dot(amat[pl.ds(pl.multiple_of(zt * 256, 256), 256), :], xr).astype(BF16)
        outt[pl.ds(zt * NP, NP)] = rows.reshape(NP, 16, 128)

        def go(j, carry2):
            d_send(i, j).start()
            return carry2

        lax.fori_loop(jnp.where(i == 0, 1, 0), NP, go, 0)
        return carry

    lax.fori_loop(0, NZ, dispatch, 0)
    rcv[c, me] = outt[me]

    def h_send(k):
        at = pl.ds(k * NP, NP)
        return push(rcv.at[c, at], rcv.at[c, at], h_s.at[k], h_r.at[k], partner)

    def land(i, carry):
        zs = (z + i) % NZ

        def take(j, carry2):
            _, s = place(i, j)
            push(rcv.at[c, s], rcv.at[c, s], d_r.at[s], d_r.at[s], partner).wait_recv()
            return carry2

        lax.fori_loop(jnp.where(i == 0, 1, 0), NP, take, 0)
        h_send(zs).start()
        return carry

    lax.fori_loop(0, NZ, land, 0)

    def unpack(side):
        xf[...] = rcv[side].astype(F32).reshape(2048, 128)
        for k in range(8):
            xm[:, pl.ds(pl.multiple_of(side * HALF + k * 128, 128), 128)] = xf[
                pl.ds(k, 256, stride=8), :
            ].astype(BF16)

    unpack(c)

    def forwarded(k, carry):
        at = pl.ds(k * NP, NP)
        push(rcv.at[1 - c, at], rcv.at[1 - c, at], h_r.at[k], h_r.at[k], partner).wait_recv()
        return carry

    lax.fori_loop(0, NZ, forwarded, 0)
    unpack(1 - c)

    for load in loads:
        load.wait()

    for lo, hi in ((0, 256), (256, 512), (512, DE)):
        gate = nn_dot(xm[...], wg[:, lo:hi])
        up = nn_dot(xm[...], wu[:, lo:hi])
        hid[:, lo:hi] = (gate * jax.nn.sigmoid(gate) * up).astype(BF16)

    def down(k, carry):
        for s in range(2):
            part2 = nn_dot(hid[...], wd[:, pl.ds(pl.multiple_of(s * HALF + k * 256, 256), 256)])
            pd[s, :, pl.ds(pl.multiple_of(k * 256, 256), 256)] = part2.astype(BF16)
        return carry

    lax.fori_loop(0, 4, down, 0)

    trade = push(pd.at[1 - c], pd_ot, k_s, k_r, partner)
    trade.start()
    trade.wait_recv()
    for k in range(8):
        at = slice(k * 128, (k + 1) * 128)
        xf[pl.ds(k, 256, stride=8), :] = pd[c, :, at].astype(F32) + pd_ot[:, at].astype(F32)
    back[...] = xf[...].astype(BF16).reshape(128, 16, 128)

    def b_send(i, j):
        to, s = place(i, j)
        return push(back.at[s], ret.at[me], b_s.at[s], b_r.at[me], to)

    over_peers(lambda i, j: b_send(i, j).start())
    ret[me] = back[me]

    def b_wait(i, j):
        _, s = place(i, j)
        push(ret.at[s], ret.at[s], b_r.at[s], b_r.at[s], partner).wait_recv()

    over_peers(b_wait)

    rows = ret[...].reshape(2048, 128)
    weighted = nn_dot(whi[...], rows) + nn_dot(wlo[...], rows)
    for k in range(8):
        mixed_ref[:, cols(k)] = (
            resid[:, cols(k)].astype(F32) + weighted[ROWS * k:ROWS * (k + 1)]
        ).astype(BF16)
    last = push(mixed_ref.at[:, half], mixed_ref.at[:, half], m_s, m_r, partner)
    last.start()
    push(mixed_ref.at[:, other], mixed_ref.at[:, other], m_s, m_r, partner).wait_recv()

    last.wait_send()
    swap.wait_send()
    trade.wait_send()

    def h_sent(k, carry):
        h_send(k).wait_send()
        return carry

    lax.fori_loop(0, NZ, h_sent, 0)

    def sent(i, j):
        d_send(i, j).wait_send()
        b_send(i, j).wait_send()

    over_peers(sent)


def experts(cell_out, tokens, ffn_gain, wof, crow, ccol, wcol, wg, wu, wd):
    dma = pltpu.SemaphoreType.DMA
    vm = pl.BlockSpec(memory_space=pltpu.VMEM)
    hbm = pl.BlockSpec(memory_space=pl.ANY)
    return pl.pallas_call(
        expert_kernel,
        name="experts",
        out_shape=jax.ShapeDtypeStruct((ROWS, D), BF16),
        in_specs=[vm] * 7 + [hbm] * 3,
        out_specs=vm,
        scratch_shapes=[
            pltpu.VMEM((ROWS, D), BF16),
            pltpu.VMEM((ROWS, D), BF16),
            pltpu.VMEM((ROWS, D), BF16),
            pltpu.VMEM((ROWS, D), BF16),
            pltpu.VMEM((2048, 256), BF16),
            pltpu.VMEM((256, 2048), BF16),
            pltpu.VMEM((256, 2048), BF16),
            pltpu.VMEM((128, 16, 128), BF16),
            pltpu.VMEM((2, 128, 16, 128), BF16),
            pltpu.VMEM((2048, 128), F32),
            pltpu.VMEM((256, D), BF16),
            pltpu.VMEM((D, DE), BF16),
            pltpu.VMEM((D, DE), BF16),
            pltpu.VMEM((DE, D), BF16),
            pltpu.VMEM((256, DE), BF16),
            pltpu.VMEM((2, 256, HALF), BF16),
            pltpu.VMEM((256, HALF), BF16),
            pltpu.VMEM((128, 16, 128), BF16),
            pltpu.VMEM((128, 16, 128), BF16),
            dma((3,)),
            dma, dma,
            dma((128,)), dma((128,)),
            dma((NZ,)), dma((NZ,)),
            dma, dma,
            dma((128,)), dma((128,)),
            dma, dma,
        ],
        compiler_params=pltpu.CompilerParams(
            collective_id=1, has_side_effects=True, vmem_limit_bytes=56 << 20
        ),
    )(cell_out, tokens, ffn_gain.reshape(1, D), wof, crow, ccol, wcol, wg, wu, wd)


def memory_cell(query, key_row, value_row, outgate, input_pre, forget_pre, head_gain,
                state_matrix, state_norm, state_max):
    seq_rows, head_count = input_pre.shape
    head_size = query.shape[1] // head_count
    query_heads = query.astype(F32).reshape(seq_rows, head_count, head_size)
    key_heads = key_row.astype(F32).reshape(seq_rows, head_count, head_size) * head_size ** (-0.5)
    value_heads = value_row.astype(F32).reshape(seq_rows, head_count, head_size)
    log_forget = jax.nn.log_sigmoid(forget_pre)
    new_max = jnp.maximum(log_forget + state_max, input_pre)
    keep_old = jnp.exp(log_forget + state_max - new_max)
    keep_new = jnp.exp(input_pre - new_max)
    new_matrix = (
        keep_old[:, :, None, None] * state_matrix
        + keep_new[:, :, None, None] * value_heads[:, :, :, None] * key_heads[:, :, None, :]
    )
    new_norm = keep_old[:, :, None] * state_norm + keep_new[:, :, None] * key_heads
    numerator = jnp.einsum("bhvd,bhd->bhv", new_matrix, query_heads)
    denominator = jnp.sum(new_norm * query_heads, axis=-1)
    cell_read = numerator / jnp.maximum(jnp.abs(denominator), jnp.exp(-new_max))[:, :, None]
    centered = cell_read - jnp.mean(cell_read, axis=-1, keepdims=True)
    variance = jnp.mean(centered * centered, axis=-1, keepdims=True)
    scaled_cell = (centered * lax.rsqrt(variance + 1e-06)).reshape(seq_rows, head_count * head_size)
    cell_out = (scaled_cell * head_gain * jax.nn.sigmoid(outgate.astype(F32))).astype(BF16)
    return (cell_out, new_matrix, new_norm, new_max)


def body(tokens, mix_gain, w_query, w_key, w_value, w_outgate, w_igate, w_fgate, igate_bias,
         fgate_bias, head_gain, w_out, state_matrix, state_norm, state_max, ffn_gain,
         w_expert_gate, w_expert_up, w_expert_down, routes, route_weights):
    z = lax.axis_index("ep_0")
    main = jnp.stack((w_query, w_key, w_value, w_outgate)).reshape(4, 16, NZ, 32)
    main = main.transpose(2, 1, 0, 3).reshape(NZ, 16, 128)
    gate_cols = jnp.tile(jnp.concatenate((w_igate, w_fgate), axis=1), (1, 16))
    lane = jnp.arange(128, dtype=jnp.int32)[None, :]
    gate_tile = jnp.where(lane // 8 == z, gate_cols, jnp.zeros_like(gate_cols))
    wp = jnp.concatenate((main, jnp.broadcast_to(gate_tile[None], (NZ, 16, 128))), axis=1)
    proj, gates, wof = gather(tokens, mix_gain, wp, w_out.T)
    parts = proj.reshape(NZ, ROWS, 4, 32).transpose(2, 1, 0, 3).reshape(4, ROWS, 256)
    input_pre = gates[:, 0:4] + igate_bias
    forget_pre = gates[:, 4:8] + fgate_bias
    cell_out, new_matrix, new_norm, new_max = memory_cell(
        parts[0], parts[1], parts[2], parts[3], input_pre, forget_pre, head_gain,
        state_matrix, state_norm, state_max,
    )
    flat = routes.reshape(-1)
    owner = jnp.arange(96, dtype=jnp.int32) // 3
    same = (flat[:, None] == flat[None, :]) & (owner[None, :] < owner[:, None])
    slot = jnp.sum(same.astype(jnp.int32), axis=1)
    code = ((flat * 2 + slot) * 8).reshape(ROWS, 3)
    fb = jnp.arange(8, dtype=jnp.int32)
    crow = (code.T[:, None, :] + fb[None, :, None]).reshape(3, 256)
    ccol = (code[None, :, :] + fb[:, None, None]).reshape(256, 3)
    wcol = jnp.broadcast_to(route_weights[None], (8, ROWS, 3)).reshape(256, 3)
    mixed = experts(cell_out, tokens, ffn_gain, wof, crow, ccol, wcol,
                    w_expert_gate, w_expert_up, w_expert_down)
    return (mixed, new_matrix, new_norm, new_max)


def solution(mesh):
    torus = Mesh(mesh.devices.reshape(NZ, NY, NX, mesh.shape["tp"]), (*EP, "tp"))
    placed = (
        P(EP, None), P(), P(EP, "tp"), P(EP, "tp"), P(EP, "tp"), P(EP, "tp"), P(EP, "tp"),
        P(EP, "tp"), P("tp"), P("tp"), P("tp"), P("tp", EP), P(EP, "tp", None, None),
        P(EP, "tp", None), P(EP, "tp"), P(), P(EP, None, "tp"), P(EP, None, "tp"),
        P(EP, "tp", None), P(EP, None), P(EP, None),
    )
    return jax.shard_map(
        body,
        mesh=torus,
        in_specs=placed,
        out_specs=(P(EP, None), P(EP, "tp", None, None), P(EP, "tp", None), P(EP, "tp")),
        check_vma=False,
    )
```

```python
import jax
import jax.numpy as jnp
from jax import lax
from jax.experimental import pallas as pl
from jax.experimental.pallas import tpu as pltpu
from jax.sharding import Mesh
from jax.sharding import PartitionSpec as P

EP = ("ep_0", "ep_1", "ep_2")
NZ, NY, NX = 8, 4, 4
NP = NY * NX
D, HALF = 2048, 1024
DE = 704
ROWS = 32
MESH = pl.DeviceIdType.MESH
F32, BF16 = jnp.float32, jnp.bfloat16


def whereami():
    return (
        lax.axis_index("ep_0"),
        lax.axis_index("ep_1"),
        lax.axis_index("ep_2"),
        lax.axis_index("tp"),
    )


def push(src, dst, send_sem, recv_sem, to):
    return pltpu.make_async_remote_copy(
        src_ref=src,
        dst_ref=dst,
        send_sem=send_sem,
        recv_sem=recv_sem,
        device_id=to,
        device_id_type=MESH,
    )


def nt_dot(a, b):
    return lax.dot_general(a, b, (((1,), (1,)), ((), ())), preferred_element_type=F32)


def nn_dot(a, b):
    return jnp.dot(a, b, preferred_element_type=F32)


def rms_scale(values, gain):
    return values * lax.rsqrt(jnp.mean(values * values, axis=-1, keepdims=True) + 1e-06) * gain


ZOFF = (4, 3, 5, 2, 6, 1, 7)


def fused_kernel(
    tok_h, mg_h, wq_h, wk_h, wv_h, wg_h, ig_h, fg_h, ib_h, fb_h, hg_h, wo_h, sm_h, sn_h, fgain_h,
    rt_h, rw_h, st_h, eg_h, eu_h, ed_h,
    mixed_ref, nmat_h, nnorm_ref, nmax_ref,
    tok, mg, wq, wk, wv, wg, ig, fg, ib, fb, hg, wo, sm, sn, fgain, rt, rw, st, eg, eu, ed,
    nall, wst, gst, gtile, gsum, wfull, gt, woz, wof, res, proj, tbuf, b8,
    qrow, kcol, keep, scal, vt, cell,
    p_my, p_ot, resid, ntwo, amat, wmat, outt, rcv, xf, xm, hid, pd, pd_ot, own, yf, back, ret,
    ld, out_sem, n_r, f_s, f_r, one_s, one_r, d_r, h_s, h_r, k_r, b_r,
):
    z, y, x, c = whereami()
    yx = y * NX + x
    me = z * NP + yx
    partner = (z, y, x, 1 - c)
    half = pl.ds(pl.multiple_of(c * HALF, HALF), HALF)
    other = pl.ds(pl.multiple_of((1 - c) * HALF, HALF), HALF)

    ins = (tok_h, mg_h, wq_h, wk_h, wv_h, wg_h, ig_h, fg_h, ib_h, fb_h, hg_h, wo_h, sm_h, sn_h,
           fgain_h, rt_h, rw_h, st_h, eg_h.at[0], eu_h.at[0], ed_h.at[0])
    dsts = (tok, mg, wq, wk, wv, wg, ig, fg, ib, fb, hg, wo, sm, sn, fgain, rt, rw, st, eg, eu, ed)
    loads = [pltpu.make_async_copy(a, b, ld.at[k]) for k, (a, b) in enumerate(zip(ins, dsts))]
    for load in loads:
        load.start()

    def zpeer(d):
        return (z + d) % NZ

    def ppeer(d):
        yt, xt = (y + d // NX) % NY, (x + d % NX) % NX
        return yt, xt, yt * NX + xt

    def loop(lo, hi, body):
        def step(k, carry):
            body(k)
            return carry

        lax.fori_loop(lo, hi, step, 0)

    def place(off, j):
        zt = zpeer(off)
        yt, xt, yxt = ppeer(j)
        return (zt, yt, xt, c), zt * NP + yxt

    barrier = pltpu.get_barrier_semaphore()

    def greet_plane(off, lo):
        def greet(j):
            to, _ = place(off, j)
            pl.semaphore_signal(barrier, 1, device_id=to, device_id_type=MESH)

        loop(lo, NP, greet)

    loop(1, NZ, lambda i: greet_plane(i, 0))
    greet_plane(0, 1)
    pl.semaphore_signal(barrier, 1, device_id=partner, device_id_type=MESH)

    for load in loads[:18]:
        load.wait()

    nall[z] = rms_scale(tok[...].astype(F32), mg[...]).astype(BF16)

    tbuf[...] = jnp.zeros((128, 128), F32)
    b8[...] = jnp.zeros((8, 128), F32)
    b8[0:4, 0:16] = ig[...].astype(F32)
    b8[4:8, 0:16] = fg[...].astype(F32)
    tbuf[pl.ds(pl.multiple_of(z * 8, 8), 8), :] = b8[...]
    gtile[...] = tbuf[...].T[0:16, :].astype(BF16)

    pl.semaphore_wait(barrier, NZ * NP)

    wsrc = (wq, wk, wv, wg)

    def w_send(t):
        return push(
            wsrc[t // 2].at[:, (t % 2) * 128:(t % 2 + 1) * 128], wst.at[z],
            one_s.at[0], one_r.at[0], (t, y, x, c),
        )

    for t in range(NZ):
        @pl.when(z != t)
        def _(t=t):
            w_send(t).start()

        @pl.when(z == t)
        def _(t=t):
            wst[t] = wsrc[t // 2][:, (t % 2) * 128:(t % 2 + 1) * 128]

    def gz_send(d):
        return push(gtile, gst.at[z], one_s.at[1], one_r.at[1], (zpeer(d), y, x, c))

    def o_send(d):
        return push(wo, woz.at[z], one_s.at[2], one_r.at[2], (zpeer(d), y, x, c))

    def n_send(d):
        return push(nall.at[z, :, half], nall.at[z, :, half], one_s.at[3], n_r.at[z],
                    (zpeer(d), y, x, c))

    for d in ZOFF:
        gz_send(d).start()
    for d in ZOFF:
        n_send(d).start()
    for d in ZOFF:
        o_send(d).start()
    gst[z] = gtile[...]
    woz[z] = wo[...]

    def arrived(view, recv_sem):
        push(view, view, recv_sem, recv_sem, partner).wait_recv()

    def left(view, send_sem):
        push(view, view, send_sem, send_sem, partner).wait_send()

    arrived(wst.at[0:7], one_r.at[0])
    arrived(gst.at[0:7], one_r.at[1])
    total = gst[0].astype(F32)
    for k in range(1, NZ):
        total = total + gst[k].astype(F32)
    gsum[...] = total.astype(BF16)
    gt[yx] = gsum[...]
    for k in range(NZ):
        wfull[k, yx] = wst[k]

    def x_send(d):
        yt, xt, _ = ppeer(d)
        return push(wst, wfull.at[:, yx], one_s.at[4], one_r.at[4], (z, yt, xt, c))

    def g_send(d):
        yt, xt, _ = ppeer(d)
        return push(gsum, gt.at[yx], one_s.at[5], one_r.at[5], (z, yt, xt, c))

    def v_send(d):
        yt, xt, _ = ppeer(d)
        return push(woz, wof.at[:, yx], one_s.at[6], one_r.at[6], (z, yt, xt, c))

    loop(1, NP, lambda d: x_send(d).start())
    loop(1, NP, lambda d: g_send(d).start())

    tbuf[...] = jnp.zeros((128, 128), F32)
    tbuf[0:3, 0:32] = rt[...].astype(F32)
    tbuf[8:11, 0:32] = rw[...]
    tbuf[16:20, 0:32] = sm[...]
    side = tbuf[...].T
    smax = side[0:ROWS, 16:20]
    earlier = lax.broadcasted_iota(jnp.int32, (ROWS, ROWS), 1) < lax.broadcasted_iota(
        jnp.int32, (ROWS, ROWS), 0
    )
    lane256 = lax.broadcasted_iota(jnp.int32, (256, 128), 1)
    fbs = (lax.broadcasted_iota(jnp.int32, (256, 1), 0) // ROWS).astype(F32)
    code_cols, weight_cols = [], []
    table = jnp.zeros((256, 128), F32)
    for k in range(3):
        mine = side[0:ROWS, k:k + 1]
        count = jnp.zeros((ROWS, 1), F32)
        for k2 in range(3):
            theirs = tbuf[k2:k2 + 1, 0:ROWS]
            same = (mine == theirs) & earlier
            count = count + jnp.sum(jnp.where(same, 1.0, 0.0), axis=1, keepdims=True)
        code = (mine * 2.0 + count) * 8.0
        code_cols.append(jnp.concatenate([code] * 8, axis=0) + fbs)
        weight_cols.append(jnp.concatenate([side[0:ROWS, 8 + k:9 + k]] * 8, axis=0))
        table = table + jnp.where(lane256 == k, code_cols[k], 0.0)
    rows_t = table.T

    for i in range(8):
        at = slice(i * 256, (i + 1) * 256)
        row = (lax.broadcasted_iota(jnp.int32, (256, 256), 0) + i * 256).astype(F32)
        hit = (row == rows_t[0:1, :]) | (row == rows_t[1:2, :]) | (row == rows_t[2:3, :])
        amat[at, :] = jnp.where(hit, 1.0, 0.0).astype(BF16)
        col = (lax.broadcasted_iota(jnp.int32, (256, 256), 1) + i * 256).astype(F32)
        weight = jnp.zeros((256, 256), F32)
        for k in range(3):
            weight = weight + jnp.where(col == code_cols[k], weight_cols[k], 0.0)
        high = weight.astype(BF16)
        wmat[0:256, at] = high
        wmat[256:512, at] = (weight - high.astype(F32)).astype(BF16)

    arrived(woz.at[0:7], one_r.at[2])
    for k in range(NZ):
        wof[k, yx] = woz[k]
    loop(1, NP, lambda d: v_send(d).start())

    def f_send(zs):
        return push(nall.at[zs, :, half], nall.at[zs, :, half], f_s, f_r.at[zs], partner)

    for d in (1, 7, 2, 6, 3, 5, 4):
        zs = zpeer(d)
        arrived(nall.at[zs, :, half], n_r.at[zs])
        f_send(zs).start()

    arrived(gt.at[0:15], one_r.at[5])
    mine = nall[z]
    stacked = jnp.concatenate([mine[:, 256 * k:256 * (k + 1)] for k in range(NZ)], axis=0)
    gp = nn_dot(stacked, gt[...].reshape(256, 128))
    group = lax.broadcasted_iota(jnp.int32, (ROWS, 128), 1) // 8
    gates = jnp.zeros((ROWS, 128), F32)
    for k in range(NZ):
        gates = gates + jnp.where(group == k, gp[ROWS * k:ROWS * (k + 1)], 0.0)
    for shift in (64, 32, 16, 8):
        gates = gates + pltpu.roll(gates, shift, 1)
    input_pre = gates[:, 0:4] + ib[...]
    forget_pre = gates[:, 4:8] + fb[...]
    log_forget = jnp.minimum(forget_pre, 0.0) - jnp.log1p(jnp.exp(-jnp.abs(forget_pre)))
    new_max = jnp.maximum(log_forget + smax, input_pre)
    keep_old = jnp.exp(log_forget + smax - new_max)
    keep_new = jnp.exp(input_pre - new_max)
    floor = jnp.exp(-new_max)
    tbuf[...] = jnp.zeros((128, 128), F32)
    tbuf[0:ROWS, 0:4] = new_max
    nmax_ref[...] = tbuf[...].T[0:4, 0:ROWS]

    for d in (1, 7, 2, 6, 3, 5, 4):
        zs = zpeer(d)
        arrived(nall.at[zs, :, other], f_r.at[zs])
    arrived(wfull.at[:, 0:15], one_r.at[4])

    every = nn_dot(nall[...].reshape(NZ * ROWS, D), wfull[...].reshape(D, 128))
    res[...] = every.astype(BF16).reshape(NZ, ROWS, 128)

    def p_send(d):
        zt = zpeer(d)
        return push(res.at[zt], proj.at[z], one_s.at[7], one_r.at[7], (zt, y, x, c))

    for d in ZOFF:
        p_send(d).start()
    proj[z] = res[z]
    arrived(proj.at[0:7], one_r.at[7])

    lane = lax.broadcasted_iota(jnp.int32, (ROWS, 128), 1)
    low = lane < 64

    def spread(pair):
        return jnp.where(low, pair[0], pair[1])

    def pair_sum(v):
        return (
            jnp.sum(jnp.where(low, v, 0.0), axis=1, keepdims=True),
            jnp.sum(jnp.where(low, 0.0, v), axis=1, keepdims=True),
        )

    eye = jnp.where(
        lax.broadcasted_iota(jnp.int32, (128, 128), 0) == lax.broadcasted_iota(jnp.int32, (128, 128), 1),
        1.0, 0.0,
    ).astype(BF16)
    for p in range(2):
        q = proj[p].astype(F32)
        for h in range(2):
            qrow[2 * p + h] = q[:, 64 * h:64 * (h + 1)]
            kcol[2 * p + h] = proj[2 + p][:, 64 * h:64 * (h + 1)]
        vt[p] = nt_dot(eye, proj[4 + p]).astype(BF16)
        for h in range(2):
            n = 2 * p + h
            keep[n] = jnp.broadcast_to(keep_old[:, n:n + 1], (ROWS, 64))
            scal[n] = jnp.broadcast_to(keep_new[:, n:n + 1] * 0.125, (ROWS, 64))

    lane64 = lax.broadcasted_iota(jnp.int32, (64, 128), 1)

    def read_one(b, acc):
        done = []
        for h in range(4):
            prod = st[b, h] * qrow[h, pl.ds(b, 1), :]
            done.append(jnp.where(lane64 == b, jnp.sum(prod, axis=1, keepdims=True), acc[h]))
        return tuple(done)

    acc = lax.fori_loop(0, ROWS, read_one, tuple(jnp.zeros((64, 128), F32) for _ in range(4)))

    for p in range(2):
        q, kk, vv = proj[p].astype(F32), proj[2 + p].astype(F32) * 0.125, proj[4 + p].astype(F32)
        gate = proj[6 + p].astype(F32)
        h0, h1 = 2 * p, 2 * p + 1

        def two(v):
            return v[:, h0:h0 + 1], v[:, h1:h1 + 1]

        ko, kn = two(keep_old), two(keep_new)
        tbuf[0:64, :] = acc[h0]
        tbuf[64:128, :] = acc[h1]
        num0 = tbuf[...].T[0:ROWS, :]
        norm_in = jnp.concatenate([sn[:, h0, :], sn[:, h1, :]], axis=1)
        norm_new = spread(ko) * norm_in + spread(kn) * kk
        nnorm_ref[:, h0, :] = norm_new[:, 0:64]
        nnorm_ref[:, h1, :] = norm_new[:, 64:128]
        den = pair_sum(norm_new * q)
        kq = pair_sum(kk * q)
        fl = two(floor)
        bottom = tuple(jnp.maximum(jnp.abs(den[i]), fl[i]) for i in range(2))
        read = (spread(ko) * num0 + spread(kn) * vv * spread(kq)) / spread(bottom)
        mean = tuple(v * (1.0 / 64) for v in pair_sum(read))
        centered = read - spread(mean)
        var = tuple(v * (1.0 / 64) for v in pair_sum(centered * centered))
        scaled = centered * lax.rsqrt(spread(var) + 1e-06)
        at = slice(p * 128, (p + 1) * 128)
        cell[:, at] = (scaled * hg[:, at] * jax.nn.sigmoid(gate)).astype(BF16)

    arrived(wof.at[:, 0:15], one_r.at[6])
    p_my[...] = nt_dot(cell[...], wof[...].reshape(D, 256)).astype(BF16)
    swap = push(p_my, p_ot, one_s.at[8], one_r.at[8], partner)
    swap.start()
    swap.wait_recv()
    both = p_my[...].astype(F32) + p_ot[...].astype(F32)
    rsd = (tok[...].astype(F32) + both).astype(BF16)
    resid[...] = rsd
    ntwo[...] = rms_scale(rsd.astype(F32), fgain[...]).astype(BF16)

    def cols(s, k):
        return pl.ds(pl.multiple_of(s * HALF + k * 128, 128), 128)

    xr = jnp.concatenate([ntwo[:, cols(c, k)] for k in range(8)], axis=0)

    def d_send(off, j):
        to, e = place(off, j)
        return push(outt.at[e], rcv.at[c, me], one_s.at[9], d_r.at[z], to)

    def plane256(zt):
        return pl.ds(pl.multiple_of(zt * 256, 256), 256)

    def plane16(zt):
        return pl.ds(zt * NP, NP)

    for off in (*ZOFF, 0):
        zt = zpeer(off)
        rows = nn_dot(amat[plane256(zt), :], xr).astype(BF16)
        outt[plane16(zt)] = rows.reshape(NP, 16, 128)
        loop(1 if off == 0 else 0, NP, lambda j, off=off: d_send(off, j).start())
    rcv[c, me] = outt[me]

    def write_one(b):
        for h in range(4):
            vth = vt[h // 2, 64 * (h % 2):64 * (h % 2 + 1), :]
            pick = jnp.where(
                lax.broadcasted_iota(jnp.int32, (64, ROWS), 1) == b, vth.astype(F32), 0.0
            ).astype(BF16)
            outer = nn_dot(pick, kcol[h])
            st[b, h] = keep[h, pl.ds(b, 1), :] * st[b, h] + scal[h, pl.ds(b, 1), :] * outer

    loop(0, ROWS, write_one)
    save = pltpu.make_async_copy(st, nmat_h, out_sem)
    save.start()

    def h_view(s, zs):
        return rcv.at[s, plane16(zs)]

    def h_send(zs):
        return push(h_view(c, zs), h_view(c, zs), h_s, h_r.at[zs], partner)

    def unpack(s, zs):
        xf[...] = rcv[s, plane16(zs)].astype(F32).reshape(256, 128)
        at = pl.ds(pl.multiple_of(zs * ROWS, ROWS), ROWS)
        for k in range(8):
            xm[at, cols(s, k)] = xf[pl.ds(k, ROWS, stride=8), :].astype(BF16)

    for off in (*ZOFF, 0):
        zs = (z + NZ - off) % NZ
        if off:
            arrived(rcv.at[c, plane16(zs)], d_r.at[zs])
        else:
            arrived(rcv.at[c, 0:15], d_r.at[zs])
        h_send(zs).start()
        unpack(c, zs)
    for off in (*ZOFF, 0):
        zs = (z + NZ - off) % NZ
        arrived(h_view(1 - c, zs), h_r.at[zs])
        unpack(1 - c, zs)

    for load in loads[18:]:
        load.wait()

    for lo, hi in ((0, 256), (256, 512), (512, DE)):
        gate = nt_dot(xm[...], eg[lo:hi, :])
        up = nt_dot(xm[...], eu[lo:hi, :])
        hid[:, lo:hi] = (gate * jax.nn.sigmoid(gate) * up).astype(BF16)

    def down(s, k):
        return nn_dot(hid[...], ed[:, pl.ds(pl.multiple_of(s * HALF + k * 256, 256), 256)]).astype(BF16)

    def k_send(k):
        return push(pd.at[k], pd_ot.at[k], one_s.at[10], k_r.at[k], partner)

    for k in range(4):
        pd[k] = down(1 - c, k)
        k_send(k).start()
    for k in range(4):
        own[k] = down(c, k)
    for k in range(4):
        arrived(pd_ot.at[k], k_r.at[k])
        both = own[k].astype(F32) + pd_ot[k].astype(F32)
        for h in range(2):
            yf[pl.ds(2 * k + h, 256, stride=8), :] = both[:, 128 * h:128 * (h + 1)]

    def b_send(off, j):
        to, s = place(off, j)
        return push(back.at[s], ret.at[me], one_s.at[11], b_r.at[z], to)

    for off in (*ZOFF, 0):
        zt = zpeer(off)
        back[plane16(zt)] = yf[plane256(zt), :].astype(BF16).reshape(NP, 16, 128)
        loop(1 if off == 0 else 0, NP, lambda j, off=off: b_send(off, j).start())
    ret[me] = back[me]

    weighted = jnp.zeros((512, 128), F32)
    for off in (*ZOFF, 0):
        zs = (z + NZ - off) % NZ
        if off:
            arrived(ret.at[plane16(zs)], b_r.at[zs])
        else:
            arrived(ret.at[0:15], b_r.at[zs])
        weighted = weighted + nn_dot(wmat[:, plane256(zs)], ret[plane16(zs)].reshape(256, 128))
    for k in range(8):
        mixed_ref[:, cols(c, k)] = (
            resid[:, cols(c, k)].astype(F32)
            + (weighted[ROWS * k:ROWS * (k + 1)] + weighted[256 + ROWS * k:256 + ROWS * (k + 1)])
        ).astype(BF16)
    last = push(mixed_ref.at[:, half], mixed_ref.at[:, half], one_s.at[12], one_r.at[12], partner)
    last.start()

    left(wst.at[0:7], one_s.at[0])
    left(gst.at[0:7], one_s.at[1])
    left(woz.at[0:7], one_s.at[2])
    left(nall.at[0:7, :, half], one_s.at[3])
    left(wfull.at[:, 0:15], one_s.at[4])
    left(gt.at[0:15], one_s.at[5])
    left(wof.at[:, 0:15], one_s.at[6])
    left(res.at[0:7], one_s.at[7])
    left(p_my, one_s.at[8])
    left(outt.at[0:127], one_s.at[9])
    left(pd, one_s.at[10])
    left(back.at[0:127], one_s.at[11])
    left(nall.at[0:7, :, half], f_s)
    left(outt, h_s)
    save.wait()
    arrived(mixed_ref.at[:, other], one_r.at[12])
    last.wait_send()


def fused(*args):
    dma = pltpu.SemaphoreType.DMA
    vm = pl.BlockSpec(memory_space=pltpu.VMEM)
    hbm = pl.BlockSpec(memory_space=pl.ANY)

    def buf(shape, kind=BF16):
        return pltpu.VMEM(shape, kind)

    staged = [buf(a.shape if a.ndim < 3 or a.shape[0] != 1 else a.shape[1:], a.dtype) for a in args]
    return pl.pallas_call(
        fused_kernel,
        name="layer",
        out_shape=(
            jax.ShapeDtypeStruct((ROWS, D), BF16),
            jax.ShapeDtypeStruct((ROWS, 4, 64, 64), F32),
            jax.ShapeDtypeStruct((ROWS, 4, 64), F32),
            jax.ShapeDtypeStruct((4, ROWS), F32),
        ),
        in_specs=[hbm] * len(args),
        out_specs=(vm, hbm, vm, vm),
        scratch_shapes=[
            *staged,
            buf((NZ, ROWS, D)),
            buf((NZ, 16, 128)),
            buf((NZ, 16, 128)),
            buf((16, 128)),
            buf((16, 128)),
            buf((NZ, NP, 16, 128)),
            buf((NP, 16, 128)),
            buf((NZ, 16, 256)),
            buf((NZ, NP, 16, 256)),
            buf((NZ, ROWS, 128)),
            buf((NZ, ROWS, 128)),
            buf((128, 128), F32),
            buf((8, 128), F32),
            buf((4, ROWS, 64), F32),
            buf((4, ROWS, 64)),
            buf((4, ROWS, 64), F32),
            buf((4, ROWS, 64), F32),
            buf((2, 128, ROWS)),
            buf((ROWS, 256)),
            buf((ROWS, D)),
            buf((ROWS, D)),
            buf((ROWS, D)),
            buf((ROWS, D)),
            buf((2048, 256)),
            buf((512, 2048)),
            buf((128, 16, 128)),
            buf((2, 128, 16, 128)),
            buf((256, 128), F32),
            buf((256, D)),
            buf((256, DE)),
            buf((4, 256, 256)),
            buf((4, 256, 256)),
            buf((4, 256, 256)),
            buf((2048, 128), F32),
            buf((128, 16, 128)),
            buf((128, 16, 128)),
            dma((len(args),)),
            dma,
            dma((NZ,)),
            dma,
            dma((NZ,)),
            dma((13,)),
            dma((13,)),
            dma((NZ,)),
            dma,
            dma((NZ,)),
            dma((4,)),
            dma((NZ,)),
        ],
        compiler_params=pltpu.CompilerParams(
            collective_id=0, has_side_effects=True, vmem_limit_bytes=58 << 20
        ),
    )(*args)


def body(tokens, mix_gain, w_query, w_key, w_value, w_outgate, w_igate, w_fgate, igate_bias,
         fgate_bias, head_gain, w_out, state_matrix, state_norm, state_max, ffn_gain,
         w_expert_gate, w_expert_up, w_expert_down, routes, route_weights):
    mixed, new_matrix, new_norm, new_max = fused(
        tokens, mix_gain.reshape(1, D), w_query, w_key, w_value, w_outgate, w_igate.T, w_fgate.T,
        igate_bias.reshape(1, 4), fgate_bias.reshape(1, 4), head_gain.reshape(1, 256), w_out.T,
        state_max.T, state_norm, ffn_gain.reshape(1, D), routes.T, route_weights.T, state_matrix,
        w_expert_gate.swapaxes(1, 2), w_expert_up.swapaxes(1, 2), w_expert_down,
    )
    return (mixed, new_matrix, new_norm, new_max.T)


def solution(mesh):
    torus = Mesh(mesh.devices.reshape(NZ, NY, NX, mesh.shape["tp"]), (*EP, "tp"))
    placed = (
        P(EP, None), P(), P(EP, "tp"), P(EP, "tp"), P(EP, "tp"), P(EP, "tp"), P(EP, "tp"),
        P(EP, "tp"), P("tp"), P("tp"), P("tp"), P("tp", EP), P(EP, "tp", None, None),
        P(EP, "tp", None), P(EP, "tp"), P(), P(EP, None, "tp"), P(EP, None, "tp"),
        P(EP, "tp", None), P(EP, None), P(EP, None),
    )
    return jax.shard_map(
        body,
        mesh=torus,
        in_specs=placed,
        out_specs=(P(EP, None), P(EP, "tp", None, None), P(EP, "tp", None), P(EP, "tp")),
        check_vma=False,
    )
```

```python
import jax
import jax.numpy as jnp
from jax import lax
from jax.experimental import pallas as pl
from jax.experimental.pallas import tpu as pltpu
from jax.sharding import Mesh
from jax.sharding import PartitionSpec as P

EP = ("ep_0", "ep_1", "ep_2")
NZ, NY, NX = 8, 4, 4
NP = NY * NX
D, HALF = 2048, 1024
DE = 704
ROWS = 32
MESH = pl.DeviceIdType.MESH
F32, BF16 = jnp.float32, jnp.bfloat16


def whereami():
    return (
        lax.axis_index("ep_0"),
        lax.axis_index("ep_1"),
        lax.axis_index("ep_2"),
        lax.axis_index("tp"),
    )


def push(src, dst, send_sem, recv_sem, to):
    return pltpu.make_async_remote_copy(
        src_ref=src,
        dst_ref=dst,
        send_sem=send_sem,
        recv_sem=recv_sem,
        device_id=to,
        device_id_type=MESH,
    )


def nt_dot(a, b):
    return lax.dot_general(a, b, (((1,), (1,)), ((), ())), preferred_element_type=F32)


def nn_dot(a, b):
    return jnp.dot(a, b, preferred_element_type=F32)


def rms_scale(values, gain):
    return values * lax.rsqrt(jnp.mean(values * values, axis=-1, keepdims=True) + 1e-06) * gain


ZOFF = (4, 3, 5, 2, 6, 1, 7)
OUTS = (((ROWS, D), BF16), ((ROWS, 4, 64, 64), F32), ((ROWS, 4, 64), F32), ((4, ROWS), F32))


def fused_kernel(
    tok_h, mg_h, wq_h, wk_h, wv_h, wg_h, ig_h, fg_h, ib_h, fb_h, hg_h, wo_h, sm_h, sn_h, fgain_h,
    rt_h, rw_h, st_h, eg_h, eu_h, ed_h,
    mixed_ref, nmat_ref, nnorm_ref, nmax_ref,
    tok, mg, wq, wk, wv, wg, ig, fg, ib, fb, hg, wo, sm, sn, fgain, rt, rw, st, eg, eu, ed,
    nall, wst, gst, gtile, gsum, wfull, gt, woz, wof, res, proj, tbuf, b8,
    qrow, kcol, keep, scal, vt, cell,
    p_my, p_ot, resid, ntwo, amat, wmat, outt, rcv, xf, xm, hid, pd, pd_ot, own, yf, back, ret,
    ld, n_r, f_s, f_r, one_s, one_r, d_r, h_s, h_r, k_r, b_r,
):
    z, y, x, c = whereami()
    yx = y * NX + x
    me = z * NP + yx
    partner = (z, y, x, 1 - c)
    half = pl.ds(pl.multiple_of(c * HALF, HALF), HALF)
    other = pl.ds(pl.multiple_of((1 - c) * HALF, HALF), HALF)

    ins = (tok_h, mg_h, wq_h, wk_h, wv_h, wg_h, ig_h, fg_h, ib_h, fb_h, hg_h, wo_h, sm_h, sn_h,
           fgain_h, rt_h, rw_h, st_h, eg_h.at[0], eu_h.at[0], ed_h.at[0])
    dsts = (tok, mg, wq, wk, wv, wg, ig, fg, ib, fb, hg, wo, sm, sn, fgain, rt, rw, st, eg, eu, ed)
    loads = [pltpu.make_async_copy(a, b, ld.at[k]) for k, (a, b) in enumerate(zip(ins, dsts))]
    for load in loads:
        load.start()

    def zpeer(d):
        return (z + d) % NZ

    def ppeer(d):
        yt, xt = (y + d // NX) % NY, (x + d % NX) % NX
        return yt, xt, yt * NX + xt

    def loop(lo, hi, body):
        def step(k, carry):
            body(k)
            return carry

        lax.fori_loop(lo, hi, step, 0)

    def place(off, j):
        zt = zpeer(off)
        yt, xt, yxt = ppeer(j)
        return (zt, yt, xt, c), zt * NP + yxt

    barrier = pltpu.get_barrier_semaphore()

    for d in ZOFF:
        pl.semaphore_signal(barrier, 1, device_id=(zpeer(d), y, x, c), device_id_type=MESH)

    def greet(d):
        yt, xt, _ = ppeer(d)
        pl.semaphore_signal(barrier, 1, device_id=(z, yt, xt, c), device_id_type=MESH)

    loop(1, NP, greet)
    pl.semaphore_signal(barrier, 1, device_id=partner, device_id_type=MESH)

    for load in loads[:18]:
        load.wait()

    nall[z] = rms_scale(tok[...].astype(F32), mg[...]).astype(BF16)

    tbuf[...] = jnp.zeros((128, 128), F32)
    b8[...] = jnp.zeros((8, 128), F32)
    b8[0:4, 0:16] = ig[...].astype(F32)
    b8[4:8, 0:16] = fg[...].astype(F32)
    tbuf[pl.ds(pl.multiple_of(z * 8, 8), 8), :] = b8[...]
    gtile[...] = tbuf[...].T[0:16, :].astype(BF16)

    pl.semaphore_wait(barrier, NZ - 1 + NP - 1 + 1)

    wsrc = (wq, wk, wv, wg)

    def w_send(t):
        return push(
            wsrc[t // 2].at[:, (t % 2) * 128:(t % 2 + 1) * 128], wst.at[z],
            one_s.at[0], one_r.at[0], (t, y, x, c),
        )

    for t in range(NZ):
        @pl.when(z != t)
        def _(t=t):
            w_send(t).start()

        @pl.when(z == t)
        def _(t=t):
            wst[t] = wsrc[t // 2][:, (t % 2) * 128:(t % 2 + 1) * 128]

    def gz_send(d):
        return push(gtile, gst.at[z], one_s.at[1], one_r.at[1], (zpeer(d), y, x, c))

    def o_send(d):
        return push(wo, woz.at[z], one_s.at[2], one_r.at[2], (zpeer(d), y, x, c))

    def n_send(d):
        return push(nall.at[z, :, half], nall.at[z, :, half], one_s.at[3], n_r.at[z],
                    (zpeer(d), y, x, c))

    for d in ZOFF:
        gz_send(d).start()
    for d in ZOFF:
        o_send(d).start()
    for d in ZOFF:
        n_send(d).start()
    gst[z] = gtile[...]
    woz[z] = wo[...]

    def arrived(view, recv_sem):
        push(view, view, recv_sem, recv_sem, partner).wait_recv()

    def left(view, send_sem):
        push(view, view, send_sem, send_sem, partner).wait_send()

    arrived(wst.at[0:7], one_r.at[0])
    arrived(gst.at[0:7], one_r.at[1])
    total = gst[0].astype(F32)
    for k in range(1, NZ):
        total = total + gst[k].astype(F32)
    gsum[...] = total.astype(BF16)
    gt[yx] = gsum[...]
    for k in range(NZ):
        wfull[k, yx] = wst[k]

    def x_send(d):
        yt, xt, _ = ppeer(d)
        return push(wst, wfull.at[:, yx], one_s.at[4], one_r.at[4], (z, yt, xt, c))

    def g_send(d):
        yt, xt, _ = ppeer(d)
        return push(gsum, gt.at[yx], one_s.at[5], one_r.at[5], (z, yt, xt, c))

    def v_send(d):
        yt, xt, _ = ppeer(d)
        return push(woz, wof.at[:, yx], one_s.at[6], one_r.at[6], (z, yt, xt, c))

    loop(1, NP, lambda d: x_send(d).start())
    loop(1, NP, lambda d: g_send(d).start())

    arrived(woz.at[0:7], one_r.at[2])
    for k in range(NZ):
        wof[k, yx] = woz[k]
    loop(1, NP, lambda d: v_send(d).start())

    tbuf[...] = jnp.zeros((128, 128), F32)
    tbuf[0:3, 0:32] = rt[...].astype(F32)
    tbuf[8:11, 0:32] = rw[...]
    tbuf[16:20, 0:32] = sm[...]
    side = tbuf[...].T
    smax = side[0:ROWS, 16:20]
    earlier = lax.broadcasted_iota(jnp.int32, (ROWS, ROWS), 1) < lax.broadcasted_iota(
        jnp.int32, (ROWS, ROWS), 0
    )
    lane256 = lax.broadcasted_iota(jnp.int32, (256, 128), 1)
    fbs = (lax.broadcasted_iota(jnp.int32, (256, 1), 0) // ROWS).astype(F32)
    code_cols, weight_cols = [], []
    table = jnp.zeros((256, 128), F32)
    for k in range(3):
        mine = side[0:ROWS, k:k + 1]
        count = jnp.zeros((ROWS, 1), F32)
        for k2 in range(3):
            theirs = tbuf[k2:k2 + 1, 0:ROWS]
            same = (mine == theirs) & earlier
            count = count + jnp.sum(jnp.where(same, 1.0, 0.0), axis=1, keepdims=True)
        code = (mine * 2.0 + count) * 8.0
        code_cols.append(jnp.concatenate([code] * 8, axis=0) + fbs)
        weight_cols.append(jnp.concatenate([side[0:ROWS, 8 + k:9 + k]] * 8, axis=0))
        table = table + jnp.where(lane256 == k, code_cols[k], 0.0)
    rows_t = table.T

    for i in range(8):
        at = slice(i * 256, (i + 1) * 256)
        row = (lax.broadcasted_iota(jnp.int32, (256, 256), 0) + i * 256).astype(F32)
        hit = (row == rows_t[0:1, :]) | (row == rows_t[1:2, :]) | (row == rows_t[2:3, :])
        amat[at, :] = jnp.where(hit, 1.0, 0.0).astype(BF16)
        col = (lax.broadcasted_iota(jnp.int32, (256, 256), 1) + i * 256).astype(F32)
        weight = jnp.zeros((256, 256), F32)
        for k in range(3):
            weight = weight + jnp.where(col == code_cols[k], weight_cols[k], 0.0)
        high = weight.astype(BF16)
        wmat[0:256, at] = high
        wmat[256:512, at] = (weight - high.astype(F32)).astype(BF16)

    def f_send(zs):
        return push(nall.at[zs, :, half], nall.at[zs, :, half], f_s, f_r.at[zs], partner)

    for d in (1, 7, 2, 6, 3, 5, 4):
        zs = zpeer(d)
        arrived(nall.at[zs, :, half], n_r.at[zs])
        f_send(zs).start()

    arrived(gt.at[0:15], one_r.at[5])
    mine = nall[z]
    stacked = jnp.concatenate([mine[:, 256 * k:256 * (k + 1)] for k in range(NZ)], axis=0)
    gp = nn_dot(stacked, gt[...].reshape(256, 128))
    group = lax.broadcasted_iota(jnp.int32, (ROWS, 128), 1) // 8
    gates = jnp.zeros((ROWS, 128), F32)
    for k in range(NZ):
        gates = gates + jnp.where(group == k, gp[ROWS * k:ROWS * (k + 1)], 0.0)
    for shift in (64, 32, 16, 8):
        gates = gates + pltpu.roll(gates, shift, 1)
    input_pre = gates[:, 0:4] + ib[...]
    forget_pre = gates[:, 4:8] + fb[...]
    log_forget = jnp.minimum(forget_pre, 0.0) - jnp.log1p(jnp.exp(-jnp.abs(forget_pre)))
    new_max = jnp.maximum(log_forget + smax, input_pre)
    keep_old = jnp.exp(log_forget + smax - new_max)
    keep_new = jnp.exp(input_pre - new_max)
    floor = jnp.exp(-new_max)
    tbuf[...] = jnp.zeros((128, 128), F32)
    tbuf[0:ROWS, 0:4] = new_max
    nmax_ref[...] = tbuf[...].T[0:4, 0:ROWS]

    for d in (1, 7, 2, 6, 3, 5, 4):
        zs = zpeer(d)
        arrived(nall.at[zs, :, other], f_r.at[zs])
    arrived(wfull.at[:, 0:15], one_r.at[4])

    every = nn_dot(nall[...].reshape(NZ * ROWS, D), wfull[...].reshape(D, 128))
    res[...] = every.astype(BF16).reshape(NZ, ROWS, 128)

    def p_send(d):
        zt = zpeer(d)
        return push(res.at[zt], proj.at[z], one_s.at[7], one_r.at[7], (zt, y, x, c))

    for d in ZOFF:
        p_send(d).start()
    proj[z] = res[z]
    arrived(proj.at[0:7], one_r.at[7])

    lane = lax.broadcasted_iota(jnp.int32, (ROWS, 128), 1)
    low = lane < 64

    def spread(pair):
        return jnp.where(low, pair[0], pair[1])

    def pair_sum(v):
        return (
            jnp.sum(jnp.where(low, v, 0.0), axis=1, keepdims=True),
            jnp.sum(jnp.where(low, 0.0, v), axis=1, keepdims=True),
        )

    eye = jnp.where(
        lax.broadcasted_iota(jnp.int32, (128, 128), 0) == lax.broadcasted_iota(jnp.int32, (128, 128), 1),
        1.0, 0.0,
    ).astype(BF16)
    for p in range(2):
        q = proj[p].astype(F32)
        for h in range(2):
            qrow[2 * p + h] = q[:, 64 * h:64 * (h + 1)]
            kcol[2 * p + h] = proj[2 + p][:, 64 * h:64 * (h + 1)]
        vt[p] = nt_dot(eye, proj[4 + p]).astype(BF16)
        for h in range(2):
            n = 2 * p + h
            keep[n] = jnp.broadcast_to(keep_old[:, n:n + 1], (ROWS, 64))
            scal[n] = jnp.broadcast_to(keep_new[:, n:n + 1] * 0.125, (ROWS, 64))

    lane64 = lax.broadcasted_iota(jnp.int32, (64, 128), 1)

    def read_one(b, acc):
        done = []
        for h in range(4):
            prod = st[b, h] * qrow[h, pl.ds(b, 1), :]
            done.append(jnp.where(lane64 == b, jnp.sum(prod, axis=1, keepdims=True), acc[h]))
        return tuple(done)

    acc = lax.fori_loop(0, ROWS, read_one, tuple(jnp.zeros((64, 128), F32) for _ in range(4)))

    for p in range(2):
        q, kk, vv = proj[p].astype(F32), proj[2 + p].astype(F32) * 0.125, proj[4 + p].astype(F32)
        gate = proj[6 + p].astype(F32)
        h0, h1 = 2 * p, 2 * p + 1

        def two(v):
            return v[:, h0:h0 + 1], v[:, h1:h1 + 1]

        ko, kn = two(keep_old), two(keep_new)
        tbuf[0:64, :] = acc[h0]
        tbuf[64:128, :] = acc[h1]
        num0 = tbuf[...].T[0:ROWS, :]
        norm_in = jnp.concatenate([sn[:, h0, :], sn[:, h1, :]], axis=1)
        norm_new = spread(ko) * norm_in + spread(kn) * kk
        nnorm_ref[:, h0, :] = norm_new[:, 0:64]
        nnorm_ref[:, h1, :] = norm_new[:, 64:128]
        den = pair_sum(norm_new * q)
        kq = pair_sum(kk * q)
        fl = two(floor)
        bottom = tuple(jnp.maximum(jnp.abs(den[i]), fl[i]) for i in range(2))
        read = (spread(ko) * num0 + spread(kn) * vv * spread(kq)) / spread(bottom)
        mean = tuple(v * (1.0 / 64) for v in pair_sum(read))
        centered = read - spread(mean)
        var = tuple(v * (1.0 / 64) for v in pair_sum(centered * centered))
        scaled = centered * lax.rsqrt(spread(var) + 1e-06)
        at = slice(p * 128, (p + 1) * 128)
        cell[:, at] = (scaled * hg[:, at] * jax.nn.sigmoid(gate)).astype(BF16)

    arrived(wof.at[:, 0:15], one_r.at[6])
    p_my[...] = nt_dot(cell[...], wof[...].reshape(D, 256)).astype(BF16)
    swap = push(p_my, p_ot, one_s.at[8], one_r.at[8], partner)
    swap.start()
    swap.wait_recv()
    both = p_my[...].astype(F32) + p_ot[...].astype(F32)
    rsd = (tok[...].astype(F32) + both).astype(BF16)
    resid[...] = rsd
    ntwo[...] = rms_scale(rsd.astype(F32), fgain[...]).astype(BF16)

    def cols(s, k):
        return pl.ds(pl.multiple_of(s * HALF + k * 128, 128), 128)

    xr = jnp.concatenate([ntwo[:, cols(c, k)] for k in range(8)], axis=0)

    def d_send(off, j):
        to, e = place(off, j)
        return push(outt.at[e], rcv.at[c, me], one_s.at[9], d_r.at[z], to)

    def plane256(zt):
        return pl.ds(pl.multiple_of(zt * 256, 256), 256)

    def plane16(zt):
        return pl.ds(zt * NP, NP)

    for off in (*ZOFF, 0):
        zt = zpeer(off)
        rows = nn_dot(amat[plane256(zt), :], xr).astype(BF16)
        outt[plane16(zt)] = rows.reshape(NP, 16, 128)
        loop(1 if off == 0 else 0, NP, lambda j, off=off: d_send(off, j).start())
    rcv[c, me] = outt[me]

    def write_one(b):
        for h in range(4):
            vth = vt[h // 2, 64 * (h % 2):64 * (h % 2 + 1), :]
            pick = jnp.where(
                lax.broadcasted_iota(jnp.int32, (64, ROWS), 1) == b, vth.astype(F32), 0.0
            ).astype(BF16)
            outer = nn_dot(pick, kcol[h])
            nmat_ref[b, h] = keep[h, pl.ds(b, 1), :] * st[b, h] + scal[h, pl.ds(b, 1), :] * outer

    loop(0, ROWS, write_one)

    def h_view(s, zs):
        return rcv.at[s, plane16(zs)]

    def h_send(zs):
        return push(h_view(c, zs), h_view(c, zs), h_s, h_r.at[zs], partner)

    def unpack(s, zs):
        xf[...] = rcv[s, plane16(zs)].astype(F32).reshape(256, 128)
        at = pl.ds(pl.multiple_of(zs * ROWS, ROWS), ROWS)
        for k in range(8):
            xm[at, cols(s, k)] = xf[pl.ds(k, ROWS, stride=8), :].astype(BF16)

    for off in (*ZOFF, 0):
        zs = (z + NZ - off) % NZ
        if off:
            arrived(rcv.at[c, plane16(zs)], d_r.at[zs])
        else:
            arrived(rcv.at[c, 0:15], d_r.at[zs])
        h_send(zs).start()
        unpack(c, zs)
    for off in (*ZOFF, 0):
        zs = (z + NZ - off) % NZ
        arrived(h_view(1 - c, zs), h_r.at[zs])
        unpack(1 - c, zs)

    for load in loads[18:]:
        load.wait()

    for lo, hi in ((0, 256), (256, 512), (512, DE)):
        gate = nt_dot(xm[...], eg[lo:hi, :])
        up = nt_dot(xm[...], eu[lo:hi, :])
        hid[:, lo:hi] = (gate * jax.nn.sigmoid(gate) * up).astype(BF16)

    def down(s, k):
        return nn_dot(hid[...], ed[:, pl.ds(pl.multiple_of(s * HALF + k * 256, 256), 256)]).astype(BF16)

    def k_send(k):
        return push(pd.at[k], pd_ot.at[k], one_s.at[10], k_r.at[k], partner)

    for k in range(4):
        pd[k] = down(1 - c, k)
        k_send(k).start()
    for k in range(4):
        own[k] = down(c, k)
    for k in range(4):
        arrived(pd_ot.at[k], k_r.at[k])
        both = own[k].astype(F32) + pd_ot[k].astype(F32)
        for h in range(2):
            yf[pl.ds(2 * k + h, 256, stride=8), :] = both[:, 128 * h:128 * (h + 1)]

    def b_send(off, j):
        to, s = place(off, j)
        return push(back.at[s], ret.at[me], one_s.at[11], b_r.at[z], to)

    for off in (*ZOFF, 0):
        zt = zpeer(off)
        back[plane16(zt)] = yf[plane256(zt), :].astype(BF16).reshape(NP, 16, 128)
        loop(1 if off == 0 else 0, NP, lambda j, off=off: b_send(off, j).start())
    ret[me] = back[me]

    weighted = jnp.zeros((512, 128), F32)
    for off in (*ZOFF, 0):
        zs = (z + NZ - off) % NZ
        if off:
            arrived(ret.at[plane16(zs)], b_r.at[zs])
        else:
            arrived(ret.at[0:15], b_r.at[zs])
        weighted = weighted + nn_dot(wmat[:, plane256(zs)], ret[plane16(zs)].reshape(256, 128))
    for k in range(8):
        mixed_ref[:, cols(c, k)] = (
            resid[:, cols(c, k)].astype(F32)
            + (weighted[ROWS * k:ROWS * (k + 1)] + weighted[256 + ROWS * k:256 + ROWS * (k + 1)])
        ).astype(BF16)
    last = push(mixed_ref.at[:, half], mixed_ref.at[:, half], one_s.at[12], one_r.at[12], partner)
    last.start()

    left(wst.at[0:7], one_s.at[0])
    left(gst.at[0:7], one_s.at[1])
    left(woz.at[0:7], one_s.at[2])
    left(nall.at[0:7, :, half], one_s.at[3])
    left(wfull.at[:, 0:15], one_s.at[4])
    left(gt.at[0:15], one_s.at[5])
    left(wof.at[:, 0:15], one_s.at[6])
    left(res.at[0:7], one_s.at[7])
    left(p_my, one_s.at[8])
    left(outt.at[0:127], one_s.at[9])
    left(pd, one_s.at[10])
    left(back.at[0:127], one_s.at[11])
    left(nall.at[0:7, :, half], f_s)
    left(outt, h_s)
    arrived(mixed_ref.at[:, other], one_r.at[12])
    last.wait_send()


def store_kernel(*refs):
    n = len(OUTS)
    sems = refs[-1]
    moves = [pltpu.make_async_copy(refs[k], refs[n + k], sems.at[k]) for k in range(n)]
    for move in moves:
        move.start()
    for move in moves:
        move.wait()


def stored(*arrays):
    n = len(OUTS)
    return pl.pallas_call(
        store_kernel,
        name="store",
        out_shape=tuple(jax.ShapeDtypeStruct(shape, kind) for shape, kind in OUTS),
        in_specs=[pl.BlockSpec(memory_space=pltpu.VMEM)] * n,
        out_specs=(pl.BlockSpec(memory_space=pl.ANY),) * n,
        scratch_shapes=[pltpu.SemaphoreType.DMA((n,))],
        compiler_params=pltpu.CompilerParams(vmem_limit_bytes=8 << 20),
    )(*arrays)


def fused(*args):
    dma = pltpu.SemaphoreType.DMA
    vm = pl.BlockSpec(memory_space=pltpu.VMEM)
    hbm = pl.BlockSpec(memory_space=pltpu.HBM)

    def buf(shape, kind=BF16):
        return pltpu.VMEM(shape, kind)

    staged = [buf(a.shape if a.ndim < 3 or a.shape[0] != 1 else a.shape[1:], a.dtype) for a in args]
    return pl.pallas_call(
        fused_kernel,
        name="layer",
        out_shape=tuple(pltpu.VMEM(shape, kind) for shape, kind in OUTS),
        in_specs=[hbm] * len(args),
        out_specs=(vm, vm, vm, vm),
        scratch_shapes=[
            *staged,
            buf((NZ, ROWS, D)),
            buf((NZ, 16, 128)),
            buf((NZ, 16, 128)),
            buf((16, 128)),
            buf((16, 128)),
            buf((NZ, NP, 16, 128)),
            buf((NP, 16, 128)),
            buf((NZ, 16, 256)),
            buf((NZ, NP, 16, 256)),
            buf((NZ, ROWS, 128)),
            buf((NZ, ROWS, 128)),
            buf((128, 128), F32),
            buf((8, 128), F32),
            buf((4, ROWS, 64), F32),
            buf((4, ROWS, 64)),
            buf((4, ROWS, 64), F32),
            buf((4, ROWS, 64), F32),
            buf((2, 128, ROWS)),
            buf((ROWS, 256)),
            buf((ROWS, D)),
            buf((ROWS, D)),
            buf((ROWS, D)),
            buf((ROWS, D)),
            buf((2048, 256)),
            buf((512, 2048)),
            buf((128, 16, 128)),
            buf((2, 128, 16, 128)),
            buf((256, 128), F32),
            buf((256, D)),
            buf((256, DE)),
            buf((4, 256, 256)),
            buf((4, 256, 256)),
            buf((4, 256, 256)),
            buf((2048, 128), F32),
            buf((128, 16, 128)),
            buf((128, 16, 128)),
            dma((len(args),)),
            dma((NZ,)),
            dma,
            dma((NZ,)),
            dma((13,)),
            dma((13,)),
            dma((NZ,)),
            dma,
            dma((NZ,)),
            dma((4,)),
            dma((NZ,)),
        ],
        compiler_params=pltpu.CompilerParams(
            collective_id=0, has_side_effects=True, vmem_limit_bytes=40 << 20
        ),
    )(*(pltpu.with_memory_space_constraint(a, pltpu.HBM) for a in args))


def body(tokens, mix_gain, w_query, w_key, w_value, w_outgate, w_igate, w_fgate, igate_bias,
         fgate_bias, head_gain, w_out, state_matrix, state_norm, state_max, ffn_gain,
         w_expert_gate, w_expert_up, w_expert_down, routes, route_weights):
    mixed, new_matrix, new_norm, new_max = stored(*fused(
        tokens, mix_gain.reshape(1, D), w_query, w_key, w_value, w_outgate, w_igate.T, w_fgate.T,
        igate_bias.reshape(1, 4), fgate_bias.reshape(1, 4), head_gain.reshape(1, 256), w_out.T,
        state_max.T, state_norm, ffn_gain.reshape(1, D), routes.T, route_weights.T, state_matrix,
        w_expert_gate.swapaxes(1, 2), w_expert_up.swapaxes(1, 2), w_expert_down,
    ))
    return (mixed, new_matrix, new_norm, new_max.T)


def solution(mesh):
    torus = Mesh(mesh.devices.reshape(NZ, NY, NX, mesh.shape["tp"]), (*EP, "tp"))
    placed = (
        P(EP, None), P(), P(EP, "tp"), P(EP, "tp"), P(EP, "tp"), P(EP, "tp"), P(EP, "tp"),
        P(EP, "tp"), P("tp"), P("tp"), P("tp"), P("tp", EP), P(EP, "tp", None, None),
        P(EP, "tp", None), P(EP, "tp"), P(), P(EP, None, "tp"), P(EP, None, "tp"),
        P(EP, "tp", None), P(EP, None), P(EP, None),
    )
    return jax.shard_map(
        body,
        mesh=torus,
        in_specs=placed,
        out_specs=(P(EP, None), P(EP, "tp", None, None), P(EP, "tp", None), P(EP, "tp")),
        check_vma=False,
    )
```

```python
import jax
import jax.numpy as jnp
from jax import lax
from jax.experimental import pallas as pl
from jax.experimental.pallas import tpu as pltpu
from jax.sharding import Mesh
from jax.sharding import PartitionSpec as P

EP = ("ep_0", "ep_1", "ep_2")
NZ, NY, NX = 8, 4, 4
NP = NY * NX
D, HALF = 2048, 1024
DE = 704
ROWS = 32
MESH = pl.DeviceIdType.MESH
F32, BF16 = jnp.float32, jnp.bfloat16


def whereami():
    return (
        lax.axis_index("ep_0"),
        lax.axis_index("ep_1"),
        lax.axis_index("ep_2"),
        lax.axis_index("tp"),
    )


def push(src, dst, send_sem, recv_sem, to):
    return pltpu.make_async_remote_copy(
        src_ref=src,
        dst_ref=dst,
        send_sem=send_sem,
        recv_sem=recv_sem,
        device_id=to,
        device_id_type=MESH,
    )


def nt_dot(a, b):
    return lax.dot_general(a, b, (((1,), (1,)), ((), ())), preferred_element_type=F32)


def nn_dot(a, b):
    return jnp.dot(a, b, preferred_element_type=F32)


def rms_scale(values, gain):
    return values * lax.rsqrt(jnp.mean(values * values, axis=-1, keepdims=True) + 1e-06) * gain


ZOFF = (4, 3, 5, 2, 6, 1, 7)
JOFF = (10, 9, 11, 6, 14, 2, 8, 5, 7, 13, 15, 1, 3, 4, 12, 0)
OUTS = (((ROWS, D), BF16), ((ROWS * 256, 64), F32), ((ROWS, 4, 64), F32), ((4, ROWS), F32))


def fused_kernel(
    tok_h, mg_h, wq_h, wk_h, wv_h, wg_h, ig_h, fg_h, ib_h, fb_h, hg_h, wo_h, sm_h, sn_h, fgain_h,
    rt_h, rw_h, st_h, eg_h, eu_h, ed_h,
    mixed_ref, nmat_ref, nnorm_ref, nmax_ref,
    tok, mg, wq, wk, wv, wg, ig, fg, ib, fb, hg, wo, sm, sn, fgain, rt, rw, st, eg, eu, ed,
    stt, nall, wst, gst, gtile, gsum, wfull, gt, woz, wof, res, proj, tbuf, b8,
    qrow, kcol, keep, scal, vt, cell,
    p_my, p_ot, resid, ntwo, amat, wmat, outt, rcv, xf, xm, ga, ua, hid, pd, pd_ot, own, yf, back, ret,
    ld, n_r, n4_r, f_s, f_r, one_s, one_r, d_r, h_s, h_r, k_r, b_r,
):
    z, y, x, c = whereami()
    yx = y * NX + x
    me = z * NP + yx
    partner = (z, y, x, 1 - c)
    half = pl.ds(pl.multiple_of(c * HALF, HALF), HALF)
    other = pl.ds(pl.multiple_of((1 - c) * HALF, HALF), HALF)

    ins = (tok_h, mg_h, wq_h, wk_h, wv_h, wg_h, ig_h, fg_h, ib_h, fb_h, hg_h, wo_h, sm_h, sn_h,
           fgain_h, rt_h, rw_h, st_h, eg_h.at[0], eu_h.at[0], ed_h.at[0])
    dsts = (tok, mg, wq, wk, wv, wg, ig, fg, ib, fb, hg, wo, sm, sn, fgain, rt, rw, st, eg, eu, ed)
    loads = [pltpu.make_async_copy(a, b, ld.at[k]) for k, (a, b) in enumerate(zip(ins, dsts))]
    for load in loads:
        load.start()

    def zpeer(d):
        return (z + d) % NZ

    def ppeer(d):
        yt, xt = (y + d // NX) % NY, (x + d % NX) % NX
        return yt, xt, yt * NX + xt

    def loop(lo, hi, body):
        def step(k, carry):
            body(k)
            return carry

        lax.fori_loop(lo, hi, step, 0)

    spots = [ppeer(j) for j in range(NP)]

    def planes(body):
        def step(i, carry):
            body(i, zpeer(4 + (1 - 2 * (i % 2)) * ((i + 1) // 2)))
            return carry

        lax.fori_loop(0, NZ, step, 0)

    def send_plane(i, zt, send):
        for j in JOFF:
            yt, xt, yxt = spots[j]
            copy = send((zt, yt, xt, c), zt * NP + yxt)
            if j:
                copy.start()
            else:
                pl.when(i < NZ - 1)(copy.start)

    barrier = pltpu.get_barrier_semaphore()

    for d in ZOFF:
        pl.semaphore_signal(barrier, 1, device_id=(zpeer(d), y, x, c), device_id_type=MESH)

    def greet(d):
        yt, xt, _ = ppeer(d)
        pl.semaphore_signal(barrier, 1, device_id=(z, yt, xt, c), device_id_type=MESH)

    loop(1, NP, greet)
    pl.semaphore_signal(barrier, 1, device_id=partner, device_id_type=MESH)

    for load in loads[:17]:
        load.wait()

    nall[z] = rms_scale(tok[...].astype(F32), mg[...]).astype(BF16)

    tbuf[...] = jnp.zeros((128, 128), F32)
    b8[...] = jnp.zeros((8, 128), F32)
    b8[0:4, 0:16] = ig[...].astype(F32)
    b8[4:8, 0:16] = fg[...].astype(F32)
    tbuf[pl.ds(pl.multiple_of(z * 8, 8), 8), :] = b8[...]
    gtile[...] = tbuf[...].T[0:16, :].astype(BF16)

    pl.semaphore_wait(barrier, NZ - 1 + NP - 1 + 1)

    wsrc = (wq, wk, wv, wg)

    def w_send(t):
        return push(
            wsrc[t // 2].at[:, (t % 2) * 128:(t % 2 + 1) * 128], wst.at[z],
            one_s.at[0], one_r.at[0], (t, y, x, c),
        )

    for t in range(NZ):
        @pl.when(z != t)
        def _(t=t):
            w_send(t).start()

        @pl.when(z == t)
        def _(t=t):
            wst[t] = wsrc[t // 2][:, (t % 2) * 128:(t % 2 + 1) * 128]

    def gz_send(d):
        return push(gtile, gst.at[z], one_s.at[1], one_r.at[1], (zpeer(d), y, x, c))

    def o_send(d):
        return push(wo, woz.at[z], one_s.at[2], one_r.at[2], (zpeer(d), y, x, c))

    def n_send(d):
        return push(nall.at[z, :, half], nall.at[z, :, half], one_s.at[3], n_r.at[z],
                    (zpeer(d), y, x, c))

    def quarter(part):
        return pl.ds(pl.multiple_of(c * HALF + part * (HALF // 2), HALF // 2), HALF // 2)

    def relay(side):
        zs = zpeer(NZ - 2 * side)
        part = quarter(0 if side > 0 else 1)
        view, cut = nall.at[zs, :, half], nall.at[zs, :, part]
        n4 = n_r.at[zs] if side > 0 else n4_r
        push(view, view, one_s.at[13], n_r.at[zs], (zpeer(NZ + side), y, x, c)).start()
        push(cut, cut, one_s.at[14], n4, (zpeer(NZ + 2 * side), y, x, c)).start()

    for d in ZOFF:
        gz_send(d).start()
    for d in ZOFF:
        o_send(d).start()
    for d in (2, 6, 1, 7):
        n_send(d).start()
    gst[z] = gtile[...]
    woz[z] = wo[...]

    def arrived(view, recv_sem):
        push(view, view, recv_sem, recv_sem, partner).wait_recv()

    def left(view, send_sem):
        push(view, view, send_sem, send_sem, partner).wait_send()

    arrived(wst.at[0:7], one_r.at[0])
    arrived(gst.at[0:7], one_r.at[1])
    total = gst[0].astype(F32)
    for k in range(1, NZ):
        total = total + gst[k].astype(F32)
    gsum[...] = total.astype(BF16)
    gt[yx] = gsum[...]
    for k in range(NZ):
        wfull[k, yx] = wst[k]

    def x_send(d):
        yt, xt, _ = ppeer(d)
        return push(wst, wfull.at[:, yx], one_s.at[4], one_r.at[4], (z, yt, xt, c))

    def g_send(d):
        yt, xt, _ = ppeer(d)
        return push(gsum, gt.at[yx], one_s.at[5], one_r.at[5], (z, yt, xt, c))

    def v_send(d):
        yt, xt, _ = ppeer(d)
        return push(woz, wof.at[:, yx], one_s.at[6], one_r.at[6], (z, yt, xt, c))

    loop(1, NP, lambda d: x_send(d).start())
    loop(1, NP, lambda d: g_send(d).start())

    def f_send(zs):
        return push(nall.at[zs, :, half], nall.at[zs, :, half], f_s, f_r.at[zs], partner)

    for side in (1, -1):
        zs = zpeer(NZ - 2 * side)
        arrived(nall.at[zs, :, half], n_r.at[zs])
        relay(side)
        f_send(zs).start()

    arrived(woz.at[0:7], one_r.at[2])
    for k in range(NZ):
        wof[k, yx] = woz[k]
    loop(1, NP, lambda d: v_send(d).start())

    tbuf[...] = jnp.zeros((128, 128), F32)
    tbuf[0:3, 0:32] = rt[...].astype(F32)
    tbuf[8:11, 0:32] = rw[...]
    tbuf[16:20, 0:32] = sm[...]
    side = tbuf[...].T
    smax = side[0:ROWS, 16:20]
    earlier = lax.broadcasted_iota(jnp.int32, (ROWS, ROWS), 1) < lax.broadcasted_iota(
        jnp.int32, (ROWS, ROWS), 0
    )
    lane256 = lax.broadcasted_iota(jnp.int32, (256, 128), 1)
    fbs = (lax.broadcasted_iota(jnp.int32, (256, 1), 0) // ROWS).astype(F32)
    code_cols, weight_cols = [], []
    table = jnp.zeros((256, 128), F32)
    for k in range(3):
        mine = side[0:ROWS, k:k + 1]
        count = jnp.zeros((ROWS, 1), F32)
        for k2 in range(3):
            theirs = tbuf[k2:k2 + 1, 0:ROWS]
            same = (mine == theirs) & earlier
            count = count + jnp.sum(jnp.where(same, 1.0, 0.0), axis=1, keepdims=True)
        code = (mine * 2.0 + count) * 8.0
        code_cols.append(jnp.concatenate([code] * 8, axis=0) + fbs)
        weight_cols.append(jnp.concatenate([side[0:ROWS, 8 + k:9 + k]] * 8, axis=0))
        table = table + jnp.where(lane256 == k, code_cols[k], 0.0)
    rows_t = table.T

    for i in range(8):
        at = slice(i * 256, (i + 1) * 256)
        row = (lax.broadcasted_iota(jnp.int32, (256, 256), 0) + i * 256).astype(F32)
        hit = (row == rows_t[0:1, :]) | (row == rows_t[1:2, :]) | (row == rows_t[2:3, :])
        amat[at, :] = jnp.where(hit, 1.0, 0.0).astype(BF16)
        col = (lax.broadcasted_iota(jnp.int32, (256, 256), 1) + i * 256).astype(F32)
        weight = jnp.zeros((256, 256), F32)
        for k in range(3):
            weight = weight + jnp.where(col == code_cols[k], weight_cols[k], 0.0)
        high = weight.astype(BF16)
        wmat[0:256, at] = high
        wmat[256:512, at] = (weight - high.astype(F32)).astype(BF16)

    loads[17].wait()

    def turn(v):
        heads = [st[pl.ds(h * 64 + v, ROWS, stride=256), :] for h in range(4)]
        stt[v] = jnp.concatenate(heads, axis=0).T

    lax.fori_loop(0, 64, lambda v, carry: (turn(v), carry)[1], 0, unroll=4)

    for d in (1, 7, 3, 5, 4):
        zs = zpeer(d)
        if d == 4:
            arrived(nall.at[zs, :, quarter(0)], n_r.at[zs])
            arrived(nall.at[zs, :, quarter(1)], n4_r)
        else:
            arrived(nall.at[zs, :, half], n_r.at[zs])
        f_send(zs).start()

    arrived(gt.at[0:15], one_r.at[5])
    mine = nall[z]
    stacked = jnp.concatenate([mine[:, 256 * k:256 * (k + 1)] for k in range(NZ)], axis=0)
    gp = nn_dot(stacked, gt[...].reshape(256, 128))
    group = lax.broadcasted_iota(jnp.int32, (ROWS, 128), 1) // 8
    gates = jnp.zeros((ROWS, 128), F32)
    for k in range(NZ):
        gates = gates + jnp.where(group == k, gp[ROWS * k:ROWS * (k + 1)], 0.0)
    for shift in (64, 32, 16, 8):
        gates = gates + pltpu.roll(gates, shift, 1)
    input_pre = gates[:, 0:4] + ib[...]
    forget_pre = gates[:, 4:8] + fb[...]
    log_forget = jnp.minimum(forget_pre, 0.0) - jnp.log1p(jnp.exp(-jnp.abs(forget_pre)))
    new_max = jnp.maximum(log_forget + smax, input_pre)
    keep_old = jnp.exp(log_forget + smax - new_max)
    keep_new = jnp.exp(input_pre - new_max)
    floor = jnp.exp(-new_max)
    tbuf[...] = jnp.zeros((128, 128), F32)
    tbuf[0:ROWS, 0:4] = new_max
    nmax_ref[...] = tbuf[...].T[0:4, 0:ROWS]

    for d in (1, 7, 2, 6, 3, 5, 4):
        zs = zpeer(d)
        arrived(nall.at[zs, :, other], f_r.at[zs])
    arrived(wfull.at[:, 0:15], one_r.at[4])

    every = nn_dot(nall[...].reshape(NZ * ROWS, D), wfull[...].reshape(D, 128))
    res[...] = every.astype(BF16).reshape(NZ, ROWS, 128)

    def p_send(d):
        zt = zpeer(d)
        return push(res.at[zt], proj.at[z], one_s.at[7], one_r.at[7], (zt, y, x, c))

    for d in ZOFF:
        p_send(d).start()
    proj[z] = res[z]
    arrived(proj.at[0:7], one_r.at[7])

    lane = lax.broadcasted_iota(jnp.int32, (ROWS, 128), 1)
    low = lane < 64

    def spread(pair):
        return jnp.where(low, pair[0], pair[1])

    def pair_sum(v):
        return (
            jnp.sum(jnp.where(low, v, 0.0), axis=1, keepdims=True),
            jnp.sum(jnp.where(low, 0.0, v), axis=1, keepdims=True),
        )

    eye = jnp.where(
        lax.broadcasted_iota(jnp.int32, (128, 128), 0) == lax.broadcasted_iota(jnp.int32, (128, 128), 1),
        1.0, 0.0,
    ).astype(BF16)
    for p in range(2):
        q = proj[p].astype(F32)
        for h in range(2):
            qrow[2 * p + h] = q[:, 64 * h:64 * (h + 1)]
            kcol[2 * p + h] = proj[2 + p][:, 64 * h:64 * (h + 1)]
        vt[p] = nt_dot(eye, proj[4 + p]).astype(BF16)
        for h in range(2):
            n = 2 * p + h
            keep[n] = jnp.broadcast_to(keep_old[:, n:n + 1], (ROWS, 64))
            scal[n] = jnp.broadcast_to(keep_new[:, n:n + 1] * 0.125, (ROWS, 64))

    q_t = jnp.concatenate([qrow[h] for h in range(4)], axis=0).T
    for k in range(8):
        tbuf[8 * k:8 * k + 8, :] = jnp.sum(stt[8 * k:8 * k + 8] * q_t[None], axis=1)
    num = tbuf[0:64, :].T

    for p in range(2):
        q, kk, vv = proj[p].astype(F32), proj[2 + p].astype(F32) * 0.125, proj[4 + p].astype(F32)
        gate = proj[6 + p].astype(F32)
        h0, h1 = 2 * p, 2 * p + 1

        def two(v):
            return v[:, h0:h0 + 1], v[:, h1:h1 + 1]

        ko, kn = two(keep_old), two(keep_new)
        num0 = jnp.concatenate(
            [num[ROWS * h0:ROWS * (h0 + 1)], num[ROWS * h1:ROWS * (h1 + 1)]], axis=1
        )
        norm_in = jnp.concatenate([sn[:, h0, :], sn[:, h1, :]], axis=1)
        norm_new = spread(ko) * norm_in + spread(kn) * kk
        nnorm_ref[:, h0, :] = norm_new[:, 0:64]
        nnorm_ref[:, h1, :] = norm_new[:, 64:128]
        den = pair_sum(norm_new * q)
        kq = pair_sum(kk * q)
        fl = two(floor)
        bottom = tuple(jnp.maximum(jnp.abs(den[i]), fl[i]) for i in range(2))
        read = (spread(ko) * num0 + spread(kn) * vv * spread(kq)) / spread(bottom)
        mean = tuple(v * (1.0 / 64) for v in pair_sum(read))
        centered = read - spread(mean)
        var = tuple(v * (1.0 / 64) for v in pair_sum(centered * centered))
        scaled = centered * lax.rsqrt(spread(var) + 1e-06)
        at = slice(p * 128, (p + 1) * 128)
        cell[:, at] = (scaled * hg[:, at] * jax.nn.sigmoid(gate)).astype(BF16)

    arrived(wof.at[:, 0:15], one_r.at[6])
    p_my[...] = nt_dot(cell[...], wof[...].reshape(D, 256)).astype(BF16)
    swap = push(p_my, p_ot, one_s.at[8], one_r.at[8], partner)
    swap.start()
    swap.wait_recv()
    both = p_my[...].astype(F32) + p_ot[...].astype(F32)
    rsd = (tok[...].astype(F32) + both).astype(BF16)
    resid[...] = rsd
    ntwo[...] = rms_scale(rsd.astype(F32), fgain[...]).astype(BF16)

    def cols(s, k):
        return pl.ds(pl.multiple_of(s * HALF + k * 128, 128), 128)

    xr = jnp.concatenate([ntwo[:, cols(c, k)] for k in range(8)], axis=0)

    def d_send(to, e):
        return push(outt.at[e], rcv.at[c, me], one_s.at[9], d_r.at[z], to)

    def plane256(zt):
        return pl.ds(pl.multiple_of(zt * 256, 256), 256)

    def plane16(zt):
        return pl.ds(zt * NP, NP)

    def dispatch(i, zt):
        rows = nn_dot(amat[plane256(zt), :], xr).astype(BF16)
        outt[plane16(zt)] = rows.reshape(NP, 16, 128)
        send_plane(i, zt, d_send)

    planes(dispatch)
    rcv[c, me] = outt[me]

    def write_one(b):
        for h in range(4):
            vth = vt[h // 2, 64 * (h % 2):64 * (h % 2 + 1), :]
            pick = jnp.where(
                lax.broadcasted_iota(jnp.int32, (64, ROWS), 1) == b, vth.astype(F32), 0.0
            ).astype(BF16)
            outer = nn_dot(pick, kcol[h])
            at = pl.ds(pl.multiple_of((b * 4 + h) * 64, 64), 64)
            nmat_ref[at, :] = keep[h, pl.ds(b, 1), :] * st[at, :] + scal[h, pl.ds(b, 1), :] * outer

    loop(0, ROWS, write_one)

    def h_view(s, zs):
        return rcv.at[s, plane16(zs)]

    def h_send(zs):
        return push(h_view(c, zs), h_view(c, zs), h_s, h_r.at[zs], partner)

    def unpack(s, zs):
        xf[...] = rcv[s, plane16(zs)].astype(F32).reshape(256, 128)
        at = pl.ds(pl.multiple_of(zs * ROWS, ROWS), ROWS)
        for k in range(8):
            xm[at, cols(s, k)] = xf[pl.ds(k, ROWS, stride=8), :].astype(BF16)

    for off in (*ZOFF, 0):
        zs = (z + NZ - off) % NZ
        if off:
            arrived(rcv.at[c, plane16(zs)], d_r.at[zs])
        else:
            arrived(rcv.at[c, 0:15], d_r.at[zs])
        h_send(zs).start()
        unpack(c, zs)
    for load in loads[18:]:
        load.wait()

    parts = ((0, 256), (256, 512), (512, DE))
    for lo, hi in parts:
        ga[:, lo:hi] = nt_dot(xm[:, half], eg[lo:hi, half])
        ua[:, lo:hi] = nt_dot(xm[:, half], eu[lo:hi, half])

    for off in (*ZOFF, 0):
        zs = (z + NZ - off) % NZ
        arrived(h_view(1 - c, zs), h_r.at[zs])
        unpack(1 - c, zs)

    for lo, hi in parts:
        gate = ga[:, lo:hi] + nt_dot(xm[:, other], eg[lo:hi, other])
        up = ua[:, lo:hi] + nt_dot(xm[:, other], eu[lo:hi, other])
        hid[:, lo:hi] = (gate * jax.nn.sigmoid(gate) * up).astype(BF16)

    def down(s, k):
        return nn_dot(hid[...], ed[:, pl.ds(pl.multiple_of(s * HALF + k * 256, 256), 256)]).astype(BF16)

    def k_send(k):
        return push(pd.at[k], pd_ot.at[k], one_s.at[10], k_r.at[k], partner)

    for k in range(4):
        pd[k] = down(1 - c, k)
        k_send(k).start()
    for k in range(4):
        own[k] = down(c, k)
    for k in range(4):
        arrived(pd_ot.at[k], k_r.at[k])
        both = own[k].astype(F32) + pd_ot[k].astype(F32)
        for h in range(2):
            yf[pl.ds(2 * k + h, 256, stride=8), :] = both[:, 128 * h:128 * (h + 1)]

    def b_send(to, s):
        return push(back.at[s], ret.at[me], one_s.at[11], b_r.at[z], to)

    def give_back(i, zt):
        back[plane16(zt)] = yf[plane256(zt), :].astype(BF16).reshape(NP, 16, 128)
        send_plane(i, zt, b_send)

    planes(give_back)
    ret[me] = back[me]

    weighted = jnp.zeros((512, 128), F32)
    for off in (*ZOFF, 0):
        zs = (z + NZ - off) % NZ
        if off:
            arrived(ret.at[plane16(zs)], b_r.at[zs])
        else:
            arrived(ret.at[0:15], b_r.at[zs])
        weighted = weighted + nn_dot(wmat[:, plane256(zs)], ret[plane16(zs)].reshape(256, 128))
    for k in range(8):
        mixed_ref[:, cols(c, k)] = (
            resid[:, cols(c, k)].astype(F32)
            + (weighted[ROWS * k:ROWS * (k + 1)] + weighted[256 + ROWS * k:256 + ROWS * (k + 1)])
        ).astype(BF16)
    last = push(mixed_ref.at[:, half], mixed_ref.at[:, half], one_s.at[12], one_r.at[12], partner)
    last.start()

    left(wst.at[0:7], one_s.at[0])
    left(gst.at[0:7], one_s.at[1])
    left(woz.at[0:7], one_s.at[2])
    left(nall.at[0:4, :, half], one_s.at[3])
    left(nall.at[0:2, :, half], one_s.at[13])
    left(nall.at[0:1, :, half], one_s.at[14])
    left(wfull.at[:, 0:15], one_s.at[4])
    left(gt.at[0:15], one_s.at[5])
    left(wof.at[:, 0:15], one_s.at[6])
    left(res.at[0:7], one_s.at[7])
    left(p_my, one_s.at[8])
    left(outt.at[0:127], one_s.at[9])
    left(pd, one_s.at[10])
    left(back.at[0:127], one_s.at[11])
    left(nall.at[0:7, :, half], f_s)
    left(outt, h_s)
    arrived(mixed_ref.at[:, other], one_r.at[12])
    last.wait_send()


PIECES = 8


def store_kernel(*refs):
    n = len(OUTS)
    sems = refs[-1]
    step = ROWS * 256 // PIECES
    pairs = [(refs[1].at[k * step:(k + 1) * step], refs[n + 1].at[k * step:(k + 1) * step]) for k in range(PIECES)]
    pairs += [(refs[k], refs[n + k]) for k in (0, 2, 3)]
    moves = [pltpu.make_async_copy(a, b, sems.at[k]) for k, (a, b) in enumerate(pairs)]
    for move in moves:
        move.start()
    for move in moves:
        move.wait()


def stored(*arrays):
    n = len(OUTS)
    return pl.pallas_call(
        store_kernel,
        name="store",
        out_shape=tuple(jax.ShapeDtypeStruct(shape, kind) for shape, kind in OUTS),
        in_specs=[pl.BlockSpec(memory_space=pltpu.VMEM)] * n,
        out_specs=(pl.BlockSpec(memory_space=pl.ANY),) * n,
        scratch_shapes=[pltpu.SemaphoreType.DMA((n - 1 + PIECES,))],
        compiler_params=pltpu.CompilerParams(vmem_limit_bytes=8 << 20),
    )(*arrays)


def fused(*args):
    dma = pltpu.SemaphoreType.DMA
    vm = pl.BlockSpec(memory_space=pltpu.VMEM)
    hbm = pl.BlockSpec(memory_space=pltpu.HBM)

    def buf(shape, kind=BF16):
        return pltpu.VMEM(shape, kind)

    staged = [buf(a.shape if a.ndim < 3 or a.shape[0] != 1 else a.shape[1:], a.dtype) for a in args]
    return pl.pallas_call(
        fused_kernel,
        name="layer",
        out_shape=tuple(pltpu.VMEM(shape, kind) for shape, kind in OUTS),
        in_specs=[hbm] * len(args),
        out_specs=(vm, vm, vm, vm),
        scratch_shapes=[
            *staged,
            buf((64, 64, 128), F32),
            buf((NZ, ROWS, D)),
            buf((NZ, 16, 128)),
            buf((NZ, 16, 128)),
            buf((16, 128)),
            buf((16, 128)),
            buf((NZ, NP, 16, 128)),
            buf((NP, 16, 128)),
            buf((NZ, 16, 256)),
            buf((NZ, NP, 16, 256)),
            buf((NZ, ROWS, 128)),
            buf((NZ, ROWS, 128)),
            buf((128, 128), F32),
            buf((8, 128), F32),
            buf((4, ROWS, 64), F32),
            buf((4, ROWS, 64)),
            buf((4, ROWS, 64), F32),
            buf((4, ROWS, 64), F32),
            buf((2, 128, ROWS)),
            buf((ROWS, 256)),
            buf((ROWS, D)),
            buf((ROWS, D)),
            buf((ROWS, D)),
            buf((ROWS, D)),
            buf((2048, 256)),
            buf((512, 2048)),
            buf((128, 16, 128)),
            buf((2, 128, 16, 128)),
            buf((256, 128), F32),
            buf((256, D)),
            buf((256, DE), F32),
            buf((256, DE), F32),
            buf((256, DE)),
            buf((4, 256, 256)),
            buf((4, 256, 256)),
            buf((4, 256, 256)),
            buf((2048, 128), F32),
            buf((128, 16, 128)),
            buf((128, 16, 128)),
            dma((len(args),)),
            dma((NZ,)),
            dma,
            dma,
            dma((NZ,)),
            dma((15,)),
            dma((15,)),
            dma((NZ,)),
            dma,
            dma((NZ,)),
            dma((4,)),
            dma((NZ,)),
        ],
        compiler_params=pltpu.CompilerParams(
            collective_id=0, has_side_effects=True, vmem_limit_bytes=40 << 20
        ),
    )(*(pltpu.with_memory_space_constraint(a, pltpu.HBM) for a in args))


def body(tokens, mix_gain, w_query, w_key, w_value, w_outgate, w_igate, w_fgate, igate_bias,
         fgate_bias, head_gain, w_out, state_matrix, state_norm, state_max, ffn_gain,
         w_expert_gate, w_expert_up, w_expert_down, routes, route_weights):
    mixed, new_matrix, new_norm, new_max = stored(*fused(
        tokens, mix_gain.reshape(1, D), w_query, w_key, w_value, w_outgate, w_igate.T, w_fgate.T,
        igate_bias.reshape(1, 4), fgate_bias.reshape(1, 4), head_gain.reshape(1, 256), w_out.T,
        state_max.T, state_norm, ffn_gain.reshape(1, D), routes.T, route_weights.T, state_matrix.reshape(ROWS * 256, 64),
        w_expert_gate.swapaxes(1, 2), w_expert_up.swapaxes(1, 2), w_expert_down,
    ))
    return (mixed, new_matrix.reshape(ROWS, 4, 64, 64), new_norm, new_max.T)


def solution(mesh):
    torus = Mesh(mesh.devices.reshape(NZ, NY, NX, mesh.shape["tp"]), (*EP, "tp"))
    placed = (
        P(EP, None), P(), P(EP, "tp"), P(EP, "tp"), P(EP, "tp"), P(EP, "tp"), P(EP, "tp"),
        P(EP, "tp"), P("tp"), P("tp"), P("tp"), P("tp", EP), P(EP, "tp", None, None),
        P(EP, "tp", None), P(EP, "tp"), P(), P(EP, None, "tp"), P(EP, None, "tp"),
        P(EP, "tp", None), P(EP, None), P(EP, None),
    )
    return jax.shard_map(
        body,
        mesh=torus,
        in_specs=placed,
        out_specs=(P(EP, None), P(EP, "tp", None, None), P(EP, "tp", None), P(EP, "tp")),
        check_vma=False,
    )
```

```python
import jax
import jax.numpy as jnp
from jax import lax
from jax.experimental import pallas as pl
from jax.experimental.pallas import tpu as pltpu
from jax.sharding import Mesh
from jax.sharding import PartitionSpec as P

EP = ("ep_0", "ep_1", "ep_2")
NZ, NY, NX = 8, 4, 4
NP = NY * NX
D, HALF = 2048, 1024
DE = 704
ROWS = 32
MESH = pl.DeviceIdType.MESH
F32, BF16 = jnp.float32, jnp.bfloat16


def whereami():
    return (
        lax.axis_index("ep_0"),
        lax.axis_index("ep_1"),
        lax.axis_index("ep_2"),
        lax.axis_index("tp"),
    )


def push(src, dst, send_sem, recv_sem, to):
    return pltpu.make_async_remote_copy(
        src_ref=src,
        dst_ref=dst,
        send_sem=send_sem,
        recv_sem=recv_sem,
        device_id=to,
        device_id_type=MESH,
    )


def nt_dot(a, b):
    return lax.dot_general(a, b, (((1,), (1,)), ((), ())), preferred_element_type=F32)


def nn_dot(a, b):
    return jnp.dot(a, b, preferred_element_type=F32)


def rms_scale(values, gain):
    return values * lax.rsqrt(jnp.mean(values * values, axis=-1, keepdims=True) + 1e-06) * gain


ZOFF = (4, 3, 5, 2, 6, 1, 7)
JOFF = (10, 9, 11, 6, 14, 2, 8, 5, 7, 13, 15, 1, 3, 4, 12, 0)
OUTS = (((ROWS, D), BF16), ((ROWS * 256, 64), F32), ((ROWS, 4, 64), F32), ((4, ROWS), F32))


def fused_kernel(
    tok_h, mg_h, wq_h, wk_h, wv_h, wg_h, ig_h, fg_h, ib_h, fb_h, hg_h, wo_h, sm_h, sn_h, fgain_h,
    rt_h, rw_h, st_h, eg_h, eu_h, ed_h,
    mixed_ref, nmat_ref, nnorm_ref, nmax_ref,
    tok, mg, wq, wk, wv, wg, ig, fg, ib, fb, hg, wo, sm, sn, fgain, rt, rw, st, eg, eu, ed,
    stt, nall, wst, gst, gtile, gsum, wfull, gt, woz, wof, wofb, res, proj, tbuf, b8,
    qrow, kcol, keep, scal, vt, cell,
    p_my, p_ot, resid, ntwo, amat, wmat, outt, rcv, xf, xm, ga, ua, hid, pd, pd_ot, own, yf, back, ret,
    ld, n_r, e_r, e4_r, f_s, f_r, one_s, one_r, d_r, h_s, h_r, k_r, b_r,
):
    z, y, x, c = whereami()
    yx = y * NX + x
    me = z * NP + yx
    partner = (z, y, x, 1 - c)
    half = pl.ds(pl.multiple_of(c * HALF, HALF), HALF)
    other = pl.ds(pl.multiple_of((1 - c) * HALF, HALF), HALF)

    ins = (tok_h, mg_h, wq_h, wk_h, wv_h, wg_h, ig_h, fg_h, ib_h, fb_h, hg_h, wo_h, sm_h, sn_h,
           fgain_h, rt_h, rw_h, st_h, eg_h.at[0], eu_h.at[0], ed_h.at[0])
    dsts = (tok, mg, wq, wk, wv, wg, ig, fg, ib, fb, hg, wo, sm, sn, fgain, rt, rw, st, eg, eu, ed)
    loads = [pltpu.make_async_copy(a, b, ld.at[k]) for k, (a, b) in enumerate(zip(ins, dsts))]
    for load in loads:
        load.start()

    def zpeer(d):
        return (z + d) % NZ

    def ppeer(d):
        yt, xt = (y + d // NX) % NY, (x + d % NX) % NX
        return yt, xt, yt * NX + xt

    def loop(lo, hi, body):
        def step(k, carry):
            body(k)
            return carry

        lax.fori_loop(lo, hi, step, 0)

    spots = [ppeer(j) for j in range(NP)]

    def planes(body):
        def step(i, carry):
            body(i, zpeer(4 + (1 - 2 * (i % 2)) * ((i + 1) // 2)))
            return carry

        lax.fori_loop(0, NZ, step, 0)

    def send_plane(i, zt, send):
        for j in JOFF:
            yt, xt, yxt = spots[j]
            copy = send((zt, yt, xt, c), zt * NP + yxt)
            if j:
                copy.start()
            else:
                pl.when(i < NZ - 1)(copy.start)

    barrier = pltpu.get_barrier_semaphore()

    for d in ZOFF:
        pl.semaphore_signal(barrier, 1, device_id=(zpeer(d), y, x, c), device_id_type=MESH)

    def greet(d):
        yt, xt, _ = ppeer(d)
        pl.semaphore_signal(barrier, 1, device_id=(z, yt, xt, c), device_id_type=MESH)

    loop(1, NP, greet)
    pl.semaphore_signal(barrier, 1, device_id=partner, device_id_type=MESH)

    for load in loads[:17]:
        load.wait()

    nall[z] = rms_scale(tok[...].astype(F32), mg[...]).astype(BF16)

    tbuf[...] = jnp.zeros((128, 128), F32)
    b8[...] = jnp.zeros((8, 128), F32)
    b8[0:4, 0:16] = ig[...].astype(F32)
    b8[4:8, 0:16] = fg[...].astype(F32)
    tbuf[pl.ds(pl.multiple_of(z * 8, 8), 8), :] = b8[...]
    gtile[...] = tbuf[...].T[0:16, :].astype(BF16)

    pl.semaphore_wait(barrier, NZ - 1 + NP - 1 + 1)

    wsrc = (wq, wk, wv, wg)

    def w_send(t):
        return push(
            wsrc[t // 2].at[:, (t % 2) * 128:(t % 2 + 1) * 128], wst.at[z],
            one_s.at[0], one_r.at[0], (t, y, x, c),
        )

    for t in range(NZ):
        @pl.when(z != t)
        def _(t=t):
            w_send(t).start()

        @pl.when(z == t)
        def _(t=t):
            wst[t] = wsrc[t // 2][:, (t % 2) * 128:(t % 2 + 1) * 128]

    def gz_send(d):
        return push(gtile, gst.at[z], one_s.at[1], one_r.at[1], (zpeer(d), y, x, c))

    def o_send(d):
        return push(wo.at[:, 0:128], woz.at[z], one_s.at[2], one_r.at[2], (zpeer(d), y, x, c))

    def e_send(d):
        yt, xt, _ = ppeer(d)
        return push(wo.at[:, 128:256], wofb.at[z, yx], one_s.at[15], one_r.at[15], (z, yt, xt, c))

    def eb_send(d):
        return push(wofb.at[z], wofb.at[z], one_s.at[16], e_r.at[z], (zpeer(d), y, x, c))

    def eb_relay(side):
        zs = zpeer(NZ - 2 * side)
        view = wofb.at[zs]
        cut = wofb.at[zs, 0:8] if side > 0 else wofb.at[zs, 8:16]
        e4 = e_r.at[zs] if side > 0 else e4_r
        push(view, view, one_s.at[17], e_r.at[zs], (zpeer(NZ + side), y, x, c)).start()
        push(cut, cut, one_s.at[18], e4, (zpeer(NZ + 2 * side), y, x, c)).start()

    def n_send(d, part):
        view = nall.at[z, :, quarter(part)]
        return push(view, view, one_s.at[3], n_r.at[part, z], (zpeer(d), y, x, c))

    def quarter(part):
        return pl.ds(pl.multiple_of(c * HALF + part * (HALF // 2), HALF // 2), HALF // 2)

    def relay(side, part):
        zs = zpeer(NZ - 2 * side)
        view = nall.at[zs, :, quarter(part)]
        push(view, view, one_s.at[13], n_r.at[part, zs], (zpeer(NZ + side), y, x, c)).start()
        if (side > 0) == (part == 0):
            push(view, view, one_s.at[14], n_r.at[part, zs], (zpeer(NZ + 2 * side), y, x, c)).start()

    for part in range(2):
        for d in (2, 6):
            n_send(d, part).start()
    for d in (1, 7):
        for part in range(2):
            n_send(d, part).start()
    for d in ZOFF:
        gz_send(d).start()
    for d in ZOFF:
        o_send(d).start()
    loop(1, NP, lambda d: e_send(d).start())
    gst[z] = gtile[...]
    woz[z] = wo[:, 0:128]
    wofb[z, yx] = wo[:, 128:256]

    def arrived(view, recv_sem):
        push(view, view, recv_sem, recv_sem, partner).wait_recv()

    def left(view, send_sem):
        push(view, view, send_sem, send_sem, partner).wait_send()

    tbuf[...] = jnp.zeros((128, 128), F32)
    tbuf[0:3, 0:32] = rt[...].astype(F32)
    tbuf[8:11, 0:32] = rw[...]
    tbuf[16:20, 0:32] = sm[...]
    side = tbuf[...].T
    smax = side[0:ROWS, 16:20]
    earlier = lax.broadcasted_iota(jnp.int32, (ROWS, ROWS), 1) < lax.broadcasted_iota(
        jnp.int32, (ROWS, ROWS), 0
    )
    lane256 = lax.broadcasted_iota(jnp.int32, (256, 128), 1)
    fbs = (lax.broadcasted_iota(jnp.int32, (256, 1), 0) // ROWS).astype(F32)
    code_cols, weight_cols = [], []
    table = jnp.zeros((256, 128), F32)
    for k in range(3):
        mine = side[0:ROWS, k:k + 1]
        count = jnp.zeros((ROWS, 1), F32)
        for k2 in range(3):
            theirs = tbuf[k2:k2 + 1, 0:ROWS]
            same = (mine == theirs) & earlier
            count = count + jnp.sum(jnp.where(same, 1.0, 0.0), axis=1, keepdims=True)
        code = (mine * 2.0 + count) * 8.0
        code_cols.append(jnp.concatenate([code] * 8, axis=0) + fbs)
        weight_cols.append(jnp.concatenate([side[0:ROWS, 8 + k:9 + k]] * 8, axis=0))
        table = table + jnp.where(lane256 == k, code_cols[k], 0.0)
    rows_t = table.T

    for i in range(8):
        at = slice(i * 256, (i + 1) * 256)
        row = (lax.broadcasted_iota(jnp.int32, (256, 256), 0) + i * 256).astype(F32)
        hit = (row == rows_t[0:1, :]) | (row == rows_t[1:2, :]) | (row == rows_t[2:3, :])
        amat[at, :] = jnp.where(hit, 1.0, 0.0).astype(BF16)
        col = (lax.broadcasted_iota(jnp.int32, (256, 256), 1) + i * 256).astype(F32)
        weight = jnp.zeros((256, 256), F32)
        for k in range(3):
            weight = weight + jnp.where(col == code_cols[k], weight_cols[k], 0.0)
        high = weight.astype(BF16)
        wmat[0:256, at] = high
        wmat[256:512, at] = (weight - high.astype(F32)).astype(BF16)

    arrived(wst.at[0:7], one_r.at[0])
    for k in range(NZ):
        wfull[k, yx] = wst[k]

    def x_send(d):
        yt, xt, _ = ppeer(d)
        return push(wst, wfull.at[:, yx], one_s.at[4], one_r.at[4], (z, yt, xt, c))

    def g_send(d):
        yt, xt, _ = ppeer(d)
        return push(gsum, gt.at[yx], one_s.at[5], one_r.at[5], (z, yt, xt, c))

    def v_send(d):
        yt, xt, _ = ppeer(d)
        return push(woz, wof.at[:, yx], one_s.at[6], one_r.at[6], (z, yt, xt, c))

    loop(1, NP, lambda d: x_send(d).start())

    def f_send(zs):
        return push(nall.at[zs, :, half], nall.at[zs, :, half], f_s, f_r.at[zs], partner)

    for part in range(2):
        for side in (1, -1):
            zs = zpeer(NZ - 2 * side)
            arrived(nall.at[zs, :, quarter(part)], n_r.at[part, zs])
            relay(side, part)
    for d in (2, 6):
        f_send(zpeer(d)).start()

    def token_in(d):
        zs = zpeer(d)
        for part in range(2):
            arrived(nall.at[zs, :, quarter(part)], n_r.at[part, zs])
        f_send(zs).start()

    for d in (1, 7):
        token_in(d)
    loads[17].wait()

    def turn(v):
        heads = [st[pl.ds(h * 64 + v, ROWS, stride=256), :] for h in range(4)]
        stt[v] = jnp.concatenate(heads, axis=0).T

    def turns(lo, hi):
        lax.fori_loop(lo, hi, lambda v, carry: (turn(v), carry)[1], 0, unroll=4)

    turns(0, 32)

    arrived(gst.at[0:7], one_r.at[1])
    total = gst[0].astype(F32)
    for k in range(1, NZ):
        total = total + gst[k].astype(F32)
    gsum[...] = total.astype(BF16)
    gt[yx] = gsum[...]
    loop(1, NP, lambda d: g_send(d).start())
    arrived(woz.at[0:7], one_r.at[2])
    for k in range(NZ):
        wof[k, yx] = woz[k]
    loop(1, NP, lambda d: v_send(d).start())

    arrived(wofb.at[0, 0:15], one_r.at[15])
    for d in (2, 6, 1, 7):
        eb_send(d).start()

    for d in (3, 5, 4):
        token_in(d)

    turns(32, 64)

    for d in (1, 7, 2, 6, 3, 5, 4):
        zs = zpeer(d)
        arrived(nall.at[zs, :, other], f_r.at[zs])
    arrived(wfull.at[:, 0:15], one_r.at[4])

    every = nn_dot(nall[...].reshape(NZ * ROWS, D), wfull[...].reshape(D, 128))
    res[...] = every.astype(BF16).reshape(NZ, ROWS, 128)

    def p_send(d):
        zt = zpeer(d)
        return push(res.at[zt], proj.at[z], one_s.at[7], one_r.at[7], (zt, y, x, c))

    for d in ZOFF:
        p_send(d).start()
    proj[z] = res[z]
    arrived(gt.at[0:15], one_r.at[5])
    mine = nall[z]
    stacked = jnp.concatenate([mine[:, 256 * k:256 * (k + 1)] for k in range(NZ)], axis=0)
    gp = nn_dot(stacked, gt[...].reshape(256, 128))
    group = lax.broadcasted_iota(jnp.int32, (ROWS, 128), 1) // 8
    gates = jnp.zeros((ROWS, 128), F32)
    for k in range(NZ):
        gates = gates + jnp.where(group == k, gp[ROWS * k:ROWS * (k + 1)], 0.0)
    for shift in (64, 32, 16, 8):
        gates = gates + pltpu.roll(gates, shift, 1)
    input_pre = gates[:, 0:4] + ib[...]
    forget_pre = gates[:, 4:8] + fb[...]
    log_forget = jnp.minimum(forget_pre, 0.0) - jnp.log1p(jnp.exp(-jnp.abs(forget_pre)))
    new_max = jnp.maximum(log_forget + smax, input_pre)
    keep_old = jnp.exp(log_forget + smax - new_max)
    keep_new = jnp.exp(input_pre - new_max)
    floor = jnp.exp(-new_max)
    tbuf[...] = jnp.zeros((128, 128), F32)
    tbuf[0:ROWS, 0:4] = new_max
    nmax_ref[...] = tbuf[...].T[0:4, 0:ROWS]

    for side in (1, -1):
        zs = zpeer(NZ - 2 * side)
        arrived(wofb.at[zs], e_r.at[zs])
        eb_relay(side)

    arrived(proj.at[0:7], one_r.at[7])

    lane = lax.broadcasted_iota(jnp.int32, (ROWS, 128), 1)
    low = lane < 64

    def spread(pair):
        return jnp.where(low, pair[0], pair[1])

    def pair_sum(v):
        return (
            jnp.sum(jnp.where(low, v, 0.0), axis=1, keepdims=True),
            jnp.sum(jnp.where(low, 0.0, v), axis=1, keepdims=True),
        )

    eye = jnp.where(
        lax.broadcasted_iota(jnp.int32, (128, 128), 0) == lax.broadcasted_iota(jnp.int32, (128, 128), 1),
        1.0, 0.0,
    ).astype(BF16)
    for p in range(2):
        q = proj[p].astype(F32)
        for h in range(2):
            qrow[2 * p + h] = q[:, 64 * h:64 * (h + 1)]
            kcol[2 * p + h] = proj[2 + p][:, 64 * h:64 * (h + 1)]
        vt[p] = nt_dot(eye, proj[4 + p]).astype(BF16)
        for h in range(2):
            n = 2 * p + h
            keep[n] = jnp.broadcast_to(keep_old[:, n:n + 1], (ROWS, 64))
            scal[n] = jnp.broadcast_to(keep_new[:, n:n + 1] * 0.125, (ROWS, 64))

    q_t = jnp.concatenate([qrow[h] for h in range(4)], axis=0).T
    for k in range(8):
        tbuf[8 * k:8 * k + 8, :] = jnp.sum(stt[8 * k:8 * k + 8] * q_t[None], axis=1)
    num = tbuf[0:64, :].T

    for p in range(2):
        q, kk, vv = proj[p].astype(F32), proj[2 + p].astype(F32) * 0.125, proj[4 + p].astype(F32)
        gate = proj[6 + p].astype(F32)
        h0, h1 = 2 * p, 2 * p + 1

        def two(v):
            return v[:, h0:h0 + 1], v[:, h1:h1 + 1]

        ko, kn = two(keep_old), two(keep_new)
        num0 = jnp.concatenate(
            [num[ROWS * h0:ROWS * (h0 + 1)], num[ROWS * h1:ROWS * (h1 + 1)]], axis=1
        )
        norm_in = jnp.concatenate([sn[:, h0, :], sn[:, h1, :]], axis=1)
        norm_new = spread(ko) * norm_in + spread(kn) * kk
        nnorm_ref[:, h0, :] = norm_new[:, 0:64]
        nnorm_ref[:, h1, :] = norm_new[:, 64:128]
        den = pair_sum(norm_new * q)
        kq = pair_sum(kk * q)
        fl = two(floor)
        bottom = tuple(jnp.maximum(jnp.abs(den[i]), fl[i]) for i in range(2))
        read = (spread(ko) * num0 + spread(kn) * vv * spread(kq)) / spread(bottom)
        mean = tuple(v * (1.0 / 64) for v in pair_sum(read))
        centered = read - spread(mean)
        var = tuple(v * (1.0 / 64) for v in pair_sum(centered * centered))
        scaled = centered * lax.rsqrt(spread(var) + 1e-06)
        at = slice(p * 128, (p + 1) * 128)
        cell[:, at] = (scaled * hg[:, at] * jax.nn.sigmoid(gate)).astype(BF16)

    arrived(wof.at[:, 0:15], one_r.at[6])
    for d in (1, 7, 3, 5, 4):
        zs = zpeer(d)
        if d == 4:
            arrived(wofb.at[zs, 0:8], e_r.at[zs])
            arrived(wofb.at[zs, 8:16], e4_r)
        else:
            arrived(wofb.at[zs], e_r.at[zs])
    p_my[...] = (
        nt_dot(cell[:, 0:128], wof[...].reshape(D, 128))
        + nt_dot(cell[:, 128:256], wofb[...].reshape(D, 128))
    ).astype(BF16)
    swap = push(p_my, p_ot, one_s.at[8], one_r.at[8], partner)
    swap.start()
    swap.wait_recv()
    both = p_my[...].astype(F32) + p_ot[...].astype(F32)
    rsd = (tok[...].astype(F32) + both).astype(BF16)
    resid[...] = rsd
    ntwo[...] = rms_scale(rsd.astype(F32), fgain[...]).astype(BF16)

    def cols(s, k):
        return pl.ds(pl.multiple_of(s * HALF + k * 128, 128), 128)

    xr = jnp.concatenate([ntwo[:, cols(c, k)] for k in range(8)], axis=0)

    def d_send(to, e):
        return push(outt.at[e], rcv.at[c, me], one_s.at[9], d_r.at[z], to)

    def plane256(zt):
        return pl.ds(pl.multiple_of(zt * 256, 256), 256)

    def plane16(zt):
        return pl.ds(zt * NP, NP)

    def dispatch(i, zt):
        rows = nn_dot(amat[plane256(zt), :], xr).astype(BF16)
        outt[plane16(zt)] = rows.reshape(NP, 16, 128)
        send_plane(i, zt, d_send)

    planes(dispatch)
    rcv[c, me] = outt[me]

    def write_one(b):
        for h in range(4):
            vth = vt[h // 2, 64 * (h % 2):64 * (h % 2 + 1), :]
            pick = jnp.where(
                lax.broadcasted_iota(jnp.int32, (64, ROWS), 1) == b, vth.astype(F32), 0.0
            ).astype(BF16)
            outer = nn_dot(pick, kcol[h])
            at = pl.ds(pl.multiple_of((b * 4 + h) * 64, 64), 64)
            nmat_ref[at, :] = keep[h, pl.ds(b, 1), :] * st[at, :] + scal[h, pl.ds(b, 1), :] * outer

    loop(0, ROWS, write_one)

    def h_view(s, zs):
        return rcv.at[s, plane16(zs)]

    def h_send(zs):
        return push(h_view(c, zs), h_view(c, zs), h_s, h_r.at[zs], partner)

    def unpack(s, zs):
        xf[...] = rcv[s, plane16(zs)].astype(F32).reshape(256, 128)
        at = pl.ds(pl.multiple_of(zs * ROWS, ROWS), ROWS)
        for k in range(8):
            xm[at, cols(s, k)] = xf[pl.ds(k, ROWS, stride=8), :].astype(BF16)

    for off in (*ZOFF, 0):
        zs = (z + NZ - off) % NZ
        if off:
            arrived(rcv.at[c, plane16(zs)], d_r.at[zs])
        else:
            arrived(rcv.at[c, 0:15], d_r.at[zs])
        h_send(zs).start()
        unpack(c, zs)
    for load in loads[18:]:
        load.wait()

    parts = ((0, 256), (256, 512), (512, DE))
    for lo, hi in parts:
        ga[:, lo:hi] = nt_dot(xm[:, half], eg[lo:hi, half])
        ua[:, lo:hi] = nt_dot(xm[:, half], eu[lo:hi, half])

    for off in (*ZOFF, 0):
        zs = (z + NZ - off) % NZ
        arrived(h_view(1 - c, zs), h_r.at[zs])
        unpack(1 - c, zs)

    for lo, hi in parts:
        gate = ga[:, lo:hi] + nt_dot(xm[:, other], eg[lo:hi, other])
        up = ua[:, lo:hi] + nt_dot(xm[:, other], eu[lo:hi, other])
        hid[:, lo:hi] = (gate * jax.nn.sigmoid(gate) * up).astype(BF16)

    def down(s, k):
        return nn_dot(hid[...], ed[:, pl.ds(pl.multiple_of(s * HALF + k * 256, 256), 256)]).astype(BF16)

    def k_send(k):
        return push(pd.at[k], pd_ot.at[k], one_s.at[10], k_r.at[k], partner)

    for k in range(4):
        pd[k] = down(1 - c, k)
        k_send(k).start()
    for k in range(4):
        own[k] = down(c, k)
    for k in range(4):
        arrived(pd_ot.at[k], k_r.at[k])
        both = own[k].astype(F32) + pd_ot[k].astype(F32)
        for h in range(2):
            yf[pl.ds(2 * k + h, 256, stride=8), :] = both[:, 128 * h:128 * (h + 1)]

    def b_send(to, s):
        return push(back.at[s], ret.at[me], one_s.at[11], b_r.at[z], to)

    def give_back(i, zt):
        back[plane16(zt)] = yf[plane256(zt), :].astype(BF16).reshape(NP, 16, 128)
        send_plane(i, zt, b_send)

    planes(give_back)
    ret[me] = back[me]

    weighted = jnp.zeros((512, 128), F32)
    for off in (*ZOFF, 0):
        zs = (z + NZ - off) % NZ
        if off:
            arrived(ret.at[plane16(zs)], b_r.at[zs])
        else:
            arrived(ret.at[0:15], b_r.at[zs])
        weighted = weighted + nn_dot(wmat[:, plane256(zs)], ret[plane16(zs)].reshape(256, 128))
    for k in range(8):
        mixed_ref[:, cols(c, k)] = (
            resid[:, cols(c, k)].astype(F32)
            + (weighted[ROWS * k:ROWS * (k + 1)] + weighted[256 + ROWS * k:256 + ROWS * (k + 1)])
        ).astype(BF16)
    last = push(mixed_ref.at[:, half], mixed_ref.at[:, half], one_s.at[12], one_r.at[12], partner)
    last.start()

    left(wst.at[0:7], one_s.at[0])
    left(gst.at[0:7], one_s.at[1])
    left(woz.at[0:7], one_s.at[2])
    left(nall.at[0:4, :, half], one_s.at[3])
    left(nall.at[0:2, :, half], one_s.at[13])
    left(nall.at[0:1, :, half], one_s.at[14])
    left(wfull.at[:, 0:15], one_s.at[4])
    left(gt.at[0:15], one_s.at[5])
    left(wof.at[:, 0:15], one_s.at[6])
    left(wofb.at[0, 0:15], one_s.at[15])
    left(wofb.at[0:4], one_s.at[16])
    left(wofb.at[0:2], one_s.at[17])
    left(wofb.at[0:1], one_s.at[18])
    left(res.at[0:7], one_s.at[7])
    left(p_my, one_s.at[8])
    left(outt.at[0:127], one_s.at[9])
    left(pd, one_s.at[10])
    left(back.at[0:127], one_s.at[11])
    left(nall.at[0:7, :, half], f_s)
    left(outt, h_s)
    arrived(mixed_ref.at[:, other], one_r.at[12])
    last.wait_send()


PIECES = 8


def store_kernel(*refs):
    n = len(OUTS)
    sems = refs[-1]
    step = ROWS * 256 // PIECES
    pairs = [(refs[1].at[k * step:(k + 1) * step], refs[n + 1].at[k * step:(k + 1) * step]) for k in range(PIECES)]
    pairs += [(refs[k], refs[n + k]) for k in (0, 2, 3)]
    moves = [pltpu.make_async_copy(a, b, sems.at[k]) for k, (a, b) in enumerate(pairs)]
    for move in moves:
        move.start()
    for move in moves:
        move.wait()


def stored(*arrays):
    n = len(OUTS)
    return pl.pallas_call(
        store_kernel,
        name="store",
        out_shape=tuple(jax.ShapeDtypeStruct(shape, kind) for shape, kind in OUTS),
        in_specs=[pl.BlockSpec(memory_space=pltpu.VMEM)] * n,
        out_specs=(pl.BlockSpec(memory_space=pl.ANY),) * n,
        scratch_shapes=[pltpu.SemaphoreType.DMA((n - 1 + PIECES,))],
        compiler_params=pltpu.CompilerParams(vmem_limit_bytes=8 << 20),
    )(*arrays)


def fused(*args):
    dma = pltpu.SemaphoreType.DMA
    vm = pl.BlockSpec(memory_space=pltpu.VMEM)
    hbm = pl.BlockSpec(memory_space=pltpu.HBM)

    def buf(shape, kind=BF16):
        return pltpu.VMEM(shape, kind)

    staged = [buf(a.shape if a.ndim < 3 or a.shape[0] != 1 else a.shape[1:], a.dtype) for a in args]
    return pl.pallas_call(
        fused_kernel,
        name="layer",
        out_shape=tuple(pltpu.VMEM(shape, kind) for shape, kind in OUTS),
        in_specs=[hbm] * len(args),
        out_specs=(vm, vm, vm, vm),
        scratch_shapes=[
            *staged,
            buf((64, 64, 128), F32),
            buf((NZ, ROWS, D)),
            buf((NZ, 16, 128)),
            buf((NZ, 16, 128)),
            buf((16, 128)),
            buf((16, 128)),
            buf((NZ, NP, 16, 128)),
            buf((NP, 16, 128)),
            buf((NZ, 16, 128)),
            buf((NZ, NP, 16, 128)),
            buf((NZ, NP, 16, 128)),
            buf((NZ, ROWS, 128)),
            buf((NZ, ROWS, 128)),
            buf((128, 128), F32),
            buf((8, 128), F32),
            buf((4, ROWS, 64), F32),
            buf((4, ROWS, 64)),
            buf((4, ROWS, 64), F32),
            buf((4, ROWS, 64), F32),
            buf((2, 128, ROWS)),
            buf((ROWS, 256)),
            buf((ROWS, D)),
            buf((ROWS, D)),
            buf((ROWS, D)),
            buf((ROWS, D)),
            buf((2048, 256)),
            buf((512, 2048)),
            buf((128, 16, 128)),
            buf((2, 128, 16, 128)),
            buf((256, 128), F32),
            buf((256, D)),
            buf((256, DE), F32),
            buf((256, DE), F32),
            buf((256, DE)),
            buf((4, 256, 256)),
            buf((4, 256, 256)),
            buf((4, 256, 256)),
            buf((2048, 128), F32),
            buf((128, 16, 128)),
            buf((128, 16, 128)),
            dma((len(args),)),
            dma((2, NZ)),
            dma((NZ,)),
            dma,
            dma,
            dma((NZ,)),
            dma((19,)),
            dma((19,)),
            dma((NZ,)),
            dma,
            dma((NZ,)),
            dma((4,)),
            dma((NZ,)),
        ],
        compiler_params=pltpu.CompilerParams(
            collective_id=0, has_side_effects=True, vmem_limit_bytes=40 << 20
        ),
    )(*(pltpu.with_memory_space_constraint(a, pltpu.HBM) for a in args))


def body(tokens, mix_gain, w_query, w_key, w_value, w_outgate, w_igate, w_fgate, igate_bias,
         fgate_bias, head_gain, w_out, state_matrix, state_norm, state_max, ffn_gain,
         w_expert_gate, w_expert_up, w_expert_down, routes, route_weights):
    mixed, new_matrix, new_norm, new_max = stored(*fused(
        tokens, mix_gain.reshape(1, D), w_query, w_key, w_value, w_outgate, w_igate.T, w_fgate.T,
        igate_bias.reshape(1, 4), fgate_bias.reshape(1, 4), head_gain.reshape(1, 256), w_out.T,
        state_max.T, state_norm, ffn_gain.reshape(1, D), routes.T, route_weights.T, state_matrix.reshape(ROWS * 256, 64),
        w_expert_gate.swapaxes(1, 2), w_expert_up.swapaxes(1, 2), w_expert_down,
    ))
    return (mixed, new_matrix.reshape(ROWS, 4, 64, 64), new_norm, new_max.T)


def solution(mesh):
    torus = Mesh(mesh.devices.reshape(NZ, NY, NX, mesh.shape["tp"]), (*EP, "tp"))
    placed = (
        P(EP, None), P(), P(EP, "tp"), P(EP, "tp"), P(EP, "tp"), P(EP, "tp"), P(EP, "tp"),
        P(EP, "tp"), P("tp"), P("tp"), P("tp"), P("tp", EP), P(EP, "tp", None, None),
        P(EP, "tp", None), P(EP, "tp"), P(), P(EP, None, "tp"), P(EP, None, "tp"),
        P(EP, "tp", None), P(EP, None), P(EP, None),
    )
    return jax.shard_map(
        body,
        mesh=torus,
        in_specs=placed,
        out_specs=(P(EP, None), P(EP, "tp", None, None), P(EP, "tp", None), P(EP, "tp")),
        check_vma=False,
    )
```

```python
import jax
import jax.numpy as jnp
from jax import lax
from jax.experimental import pallas as pl
from jax.experimental.pallas import tpu as pltpu
from jax.sharding import Mesh
from jax.sharding import PartitionSpec as P

EP = ("ep_0", "ep_1", "ep_2")
NZ, NY, NX = 8, 4, 4
NP = NY * NX
D, HALF = 2048, 1024
DE = 704
ROWS = 32
MESH = pl.DeviceIdType.MESH
F32, BF16 = jnp.float32, jnp.bfloat16


def whereami():
    return (
        lax.axis_index("ep_0"),
        lax.axis_index("ep_1"),
        lax.axis_index("ep_2"),
        lax.axis_index("tp"),
    )


def push(src, dst, send_sem, recv_sem, to):
    return pltpu.make_async_remote_copy(
        src_ref=src,
        dst_ref=dst,
        send_sem=send_sem,
        recv_sem=recv_sem,
        device_id=to,
        device_id_type=MESH,
    )


def nt_dot(a, b):
    return lax.dot_general(a, b, (((1,), (1,)), ((), ())), preferred_element_type=F32)


def nn_dot(a, b):
    return jnp.dot(a, b, preferred_element_type=F32)


def rms_scale(values, gain):
    return values * lax.rsqrt(jnp.mean(values * values, axis=-1, keepdims=True) + 1e-06) * gain


ZOFF = (4, 3, 5, 2, 6, 1, 7)
OUTS = (((ROWS, D), BF16), ((ROWS * 256, 64), F32), ((ROWS, 4, 64), F32), ((4, ROWS), F32))


def fused_kernel(
    tok_h, mg_h, wq_h, wk_h, wv_h, wg_h, ig_h, fg_h, ib_h, fb_h, hg_h, wo_h, sm_h, sn_h, fgain_h,
    rt_h, rw_h, st_h, eg_h, eu_h, ed_h,
    mixed_ref, nmat_ref, nnorm_ref, nmax_ref,
    tok, mg, wq, wk, wv, wg, ig, fg, ib, fb, hg, wo, sm, sn, fgain, rt, rw, st, eg, eu, ed,
    stt, nall, wst, gst, gtile, gsum, wfull, gt, woz, wof, wofb, res, proj, tbuf, b8,
    qrow, kcol, keep, scal, vt, cell,
    p_my, p_ot, resid, ntwo, amat, wmat, outt, rcv, xf, xm, ga, ua, hid, pd, pd_ot, own, yf, back, ret,
    ld, n_r, e_r, e4_r, f_s, f_r, one_s, one_r, d_r, h_s, h_r, k_r, b_r,
):
    z, y, x, c = whereami()
    yx = y * NX + x
    me = z * NP + yx
    partner = (z, y, x, 1 - c)
    half = pl.ds(pl.multiple_of(c * HALF, HALF), HALF)
    other = pl.ds(pl.multiple_of((1 - c) * HALF, HALF), HALF)

    ins = (tok_h, mg_h, wq_h, wk_h, wv_h, wg_h, ig_h, fg_h, ib_h, fb_h, hg_h, wo_h, sm_h, sn_h,
           fgain_h, rt_h, rw_h, st_h, eg_h.at[0], eu_h.at[0], ed_h.at[0])
    dsts = (tok, mg, wq, wk, wv, wg, ig, fg, ib, fb, hg, wo, sm, sn, fgain, rt, rw, st, eg, eu, ed)
    loads = [pltpu.make_async_copy(a, b, ld.at[k]) for k, (a, b) in enumerate(zip(ins, dsts))]
    for load in loads:
        load.start()

    def zpeer(d):
        return (z + d) % NZ

    def ppeer(d):
        yt, xt = (y + d // NX) % NY, (x + d % NX) % NX
        return yt, xt, yt * NX + xt

    def loop(lo, hi, body):
        def step(k, carry):
            body(k)
            return carry

        lax.fori_loop(lo, hi, step, 0)

    def planes(body):
        def step(i, carry):
            body(i, zpeer(4 + (1 - 2 * (i % 2)) * ((i + 1) // 2)))
            return carry

        lax.fori_loop(0, NZ, step, 0)

    def far_first(a):
        return 2 + (1 - 2 * (a % 2)) * ((a + 1) // 2)

    def send_all(send):
        def place(k):
            yt, xt = (y + far_first(k // NX)) % NY, (x + far_first(k % NX)) % NX
            for off in (*ZOFF, 0):
                zt = zpeer(off)
                copy = send((zt, yt, xt, c), zt * NP + yt * NX + xt)
                if off:
                    copy.start()
                else:
                    pl.when(k < NP - 1)(copy.start)

        loop(0, NP, place)

    barrier = pltpu.get_barrier_semaphore()

    for d in ZOFF:
        pl.semaphore_signal(barrier, 1, device_id=(zpeer(d), y, x, c), device_id_type=MESH)

    def greet(d):
        yt, xt, _ = ppeer(d)
        pl.semaphore_signal(barrier, 1, device_id=(z, yt, xt, c), device_id_type=MESH)

    loop(1, NP, greet)
    pl.semaphore_signal(barrier, 1, device_id=partner, device_id_type=MESH)

    for load in loads[:17]:
        load.wait()

    nall[z] = rms_scale(tok[...].astype(F32), mg[...]).astype(BF16)

    tbuf[...] = jnp.zeros((128, 128), F32)
    b8[...] = jnp.zeros((8, 128), F32)
    b8[0:4, 0:16] = ig[...].astype(F32)
    b8[4:8, 0:16] = fg[...].astype(F32)
    tbuf[pl.ds(pl.multiple_of(z * 8, 8), 8), :] = b8[...]
    gtile[...] = tbuf[...].T[0:16, :].astype(BF16)

    pl.semaphore_wait(barrier, NZ - 1 + NP - 1 + 1)

    wsrc = (wq, wk, wv, wg)

    def w_send(t):
        return push(
            wsrc[t // 2].at[:, (t % 2) * 128:(t % 2 + 1) * 128], wst.at[z],
            one_s.at[0], one_r.at[0], (t, y, x, c),
        )

    for t in range(NZ):
        @pl.when(z != t)
        def _(t=t):
            w_send(t).start()

        @pl.when(z == t)
        def _(t=t):
            wst[t] = wsrc[t // 2][:, (t % 2) * 128:(t % 2 + 1) * 128]

    def gz_send(d):
        return push(gtile, gst.at[z], one_s.at[1], one_r.at[1], (zpeer(d), y, x, c))

    def o_send(d):
        return push(wo.at[:, 0:128], woz.at[z], one_s.at[2], one_r.at[2], (zpeer(d), y, x, c))

    def e_send(d):
        yt, xt, _ = ppeer(d)
        return push(wo.at[:, 128:256], wofb.at[z, yx], one_s.at[15], one_r.at[15], (z, yt, xt, c))

    def eb_send(d):
        return push(wofb.at[z], wofb.at[z], one_s.at[16], e_r.at[z], (zpeer(d), y, x, c))

    def eb_relay(side):
        zs = zpeer(NZ - 2 * side)
        view = wofb.at[zs]
        cut = wofb.at[zs, 0:8] if side > 0 else wofb.at[zs, 8:16]
        e4 = e_r.at[zs] if side > 0 else e4_r
        push(view, view, one_s.at[17], e_r.at[zs], (zpeer(NZ + side), y, x, c)).start()
        push(cut, cut, one_s.at[18], e4, (zpeer(NZ + 2 * side), y, x, c)).start()

    def n_send(d, part):
        view = nall.at[z, :, quarter(part)]
        return push(view, view, one_s.at[3], n_r.at[part, z], (zpeer(d), y, x, c))

    def quarter(part):
        return pl.ds(pl.multiple_of(c * HALF + part * (HALF // 2), HALF // 2), HALF // 2)

    def relay(side, part):
        zs = zpeer(NZ - 2 * side)
        view = nall.at[zs, :, quarter(part)]
        push(view, view, one_s.at[13], n_r.at[part, zs], (zpeer(NZ + side), y, x, c)).start()
        if (side > 0) == (part == 0):
            push(view, view, one_s.at[14], n_r.at[part, zs], (zpeer(NZ + 2 * side), y, x, c)).start()

    for part in range(2):
        for d in (2, 6):
            n_send(d, part).start()
    for d in (1, 7):
        for part in range(2):
            n_send(d, part).start()
    for d in ZOFF:
        gz_send(d).start()
    for d in ZOFF:
        o_send(d).start()
    loop(1, NP, lambda d: e_send(d).start())
    gst[z] = gtile[...]
    woz[z] = wo[:, 0:128]
    wofb[z, yx] = wo[:, 128:256]

    def arrived(view, recv_sem):
        push(view, view, recv_sem, recv_sem, partner).wait_recv()

    def left(view, send_sem):
        push(view, view, send_sem, send_sem, partner).wait_send()

    tbuf[...] = jnp.zeros((128, 128), F32)
    tbuf[0:3, 0:32] = rt[...].astype(F32)
    tbuf[8:11, 0:32] = rw[...]
    tbuf[16:20, 0:32] = sm[...]
    side = tbuf[...].T
    smax = side[0:ROWS, 16:20]
    earlier = lax.broadcasted_iota(jnp.int32, (ROWS, ROWS), 1) < lax.broadcasted_iota(
        jnp.int32, (ROWS, ROWS), 0
    )
    lane256 = lax.broadcasted_iota(jnp.int32, (256, 128), 1)
    fbs = (lax.broadcasted_iota(jnp.int32, (256, 1), 0) // ROWS).astype(F32)
    code_cols, weight_cols = [], []
    table = jnp.zeros((256, 128), F32)
    for k in range(3):
        mine = side[0:ROWS, k:k + 1]
        count = jnp.zeros((ROWS, 1), F32)
        for k2 in range(3):
            theirs = tbuf[k2:k2 + 1, 0:ROWS]
            same = (mine == theirs) & earlier
            count = count + jnp.sum(jnp.where(same, 1.0, 0.0), axis=1, keepdims=True)
        code = (mine * 2.0 + count) * 8.0
        code_cols.append(jnp.concatenate([code] * 8, axis=0) + fbs)
        weight_cols.append(jnp.concatenate([side[0:ROWS, 8 + k:9 + k]] * 8, axis=0))
        table = table + jnp.where(lane256 == k, code_cols[k], 0.0)
    rows_t = table.T

    for i in range(8):
        at = slice(i * 256, (i + 1) * 256)
        row = (lax.broadcasted_iota(jnp.int32, (256, 256), 0) + i * 256).astype(F32)
        hit = (row == rows_t[0:1, :]) | (row == rows_t[1:2, :]) | (row == rows_t[2:3, :])
        amat[at, :] = jnp.where(hit, 1.0, 0.0).astype(BF16)
        col = (lax.broadcasted_iota(jnp.int32, (256, 256), 1) + i * 256).astype(F32)
        weight = jnp.zeros((256, 256), F32)
        for k in range(3):
            weight = weight + jnp.where(col == code_cols[k], weight_cols[k], 0.0)
        high = weight.astype(BF16)
        wmat[0:256, at] = high
        wmat[256:512, at] = (weight - high.astype(F32)).astype(BF16)

    arrived(wst.at[0:7], one_r.at[0])
    for k in range(NZ):
        wfull[k, yx] = wst[k]

    def x_send(d):
        yt, xt, _ = ppeer(d)
        return push(wst, wfull.at[:, yx], one_s.at[4], one_r.at[4], (z, yt, xt, c))

    def g_send(d):
        yt, xt, _ = ppeer(d)
        return push(gsum, gt.at[yx], one_s.at[5], one_r.at[5], (z, yt, xt, c))

    def v_send(d):
        yt, xt, _ = ppeer(d)
        return push(woz, wof.at[:, yx], one_s.at[6], one_r.at[6], (z, yt, xt, c))

    loop(1, NP, lambda d: x_send(d).start())

    def f_send(zs):
        return push(nall.at[zs, :, half], nall.at[zs, :, half], f_s, f_r.at[zs], partner)

    for part in range(2):
        for side in (1, -1):
            zs = zpeer(NZ - 2 * side)
            arrived(nall.at[zs, :, quarter(part)], n_r.at[part, zs])
            relay(side, part)
    for d in (2, 6):
        f_send(zpeer(d)).start()

    def token_in(d):
        zs = zpeer(d)
        for part in range(2):
            arrived(nall.at[zs, :, quarter(part)], n_r.at[part, zs])
        f_send(zs).start()

    for d in (1, 7):
        token_in(d)
    loads[17].wait()

    def turn(v):
        heads = [st[pl.ds(h * 64 + v, ROWS, stride=256), :] for h in range(4)]
        stt[v] = jnp.concatenate(heads, axis=0).T

    def turns(lo, hi):
        lax.fori_loop(lo, hi, lambda v, carry: (turn(v), carry)[1], 0, unroll=4)

    turns(0, 32)

    arrived(gst.at[0:7], one_r.at[1])
    total = gst[0].astype(F32)
    for k in range(1, NZ):
        total = total + gst[k].astype(F32)
    gsum[...] = total.astype(BF16)
    gt[yx] = gsum[...]
    loop(1, NP, lambda d: g_send(d).start())
    arrived(woz.at[0:7], one_r.at[2])
    for k in range(NZ):
        wof[k, yx] = woz[k]
    loop(1, NP, lambda d: v_send(d).start())

    arrived(wofb.at[0, 0:15], one_r.at[15])
    for d in (2, 6, 1, 7):
        eb_send(d).start()

    for d in (3, 5, 4):
        token_in(d)

    turns(32, 64)

    for d in (1, 7, 2, 6, 3, 5, 4):
        zs = zpeer(d)
        arrived(nall.at[zs, :, other], f_r.at[zs])
    arrived(wfull.at[:, 0:15], one_r.at[4])

    every = nn_dot(nall[...].reshape(NZ * ROWS, D), wfull[...].reshape(D, 128))
    res[...] = every.astype(BF16).reshape(NZ, ROWS, 128)

    def p_send(d):
        zt = zpeer(d)
        return push(res.at[zt], proj.at[z], one_s.at[7], one_r.at[7], (zt, y, x, c))

    for d in ZOFF:
        p_send(d).start()
    proj[z] = res[z]
    arrived(gt.at[0:15], one_r.at[5])
    mine = nall[z]
    stacked = jnp.concatenate([mine[:, 256 * k:256 * (k + 1)] for k in range(NZ)], axis=0)
    gp = nn_dot(stacked, gt[...].reshape(256, 128))
    group = lax.broadcasted_iota(jnp.int32, (ROWS, 128), 1) // 8
    gates = jnp.zeros((ROWS, 128), F32)
    for k in range(NZ):
        gates = gates + jnp.where(group == k, gp[ROWS * k:ROWS * (k + 1)], 0.0)
    for shift in (64, 32, 16, 8):
        gates = gates + pltpu.roll(gates, shift, 1)
    input_pre = gates[:, 0:4] + ib[...]
    forget_pre = gates[:, 4:8] + fb[...]
    log_forget = jnp.minimum(forget_pre, 0.0) - jnp.log1p(jnp.exp(-jnp.abs(forget_pre)))
    new_max = jnp.maximum(log_forget + smax, input_pre)
    keep_old = jnp.exp(log_forget + smax - new_max)
    keep_new = jnp.exp(input_pre - new_max)
    floor = jnp.exp(-new_max)
    tbuf[...] = jnp.zeros((128, 128), F32)
    tbuf[0:ROWS, 0:4] = new_max
    nmax_ref[...] = tbuf[...].T[0:4, 0:ROWS]

    for side in (1, -1):
        zs = zpeer(NZ - 2 * side)
        arrived(wofb.at[zs], e_r.at[zs])
        eb_relay(side)

    arrived(proj.at[0:7], one_r.at[7])

    lane = lax.broadcasted_iota(jnp.int32, (ROWS, 128), 1)
    low = lane < 64

    def spread(pair):
        return jnp.where(low, pair[0], pair[1])

    def pair_sum(v):
        return (
            jnp.sum(jnp.where(low, v, 0.0), axis=1, keepdims=True),
            jnp.sum(jnp.where(low, 0.0, v), axis=1, keepdims=True),
        )

    eye = jnp.where(
        lax.broadcasted_iota(jnp.int32, (128, 128), 0) == lax.broadcasted_iota(jnp.int32, (128, 128), 1),
        1.0, 0.0,
    ).astype(BF16)
    for p in range(2):
        q = proj[p].astype(F32)
        for h in range(2):
            qrow[2 * p + h] = q[:, 64 * h:64 * (h + 1)]
            kcol[2 * p + h] = proj[2 + p][:, 64 * h:64 * (h + 1)]
        vt[p] = nt_dot(eye, proj[4 + p]).astype(BF16)
        for h in range(2):
            n = 2 * p + h
            keep[n] = jnp.broadcast_to(keep_old[:, n:n + 1], (ROWS, 64))
            scal[n] = jnp.broadcast_to(keep_new[:, n:n + 1] * 0.125, (ROWS, 64))

    q_t = jnp.concatenate([qrow[h] for h in range(4)], axis=0).T
    for k in range(8):
        tbuf[8 * k:8 * k + 8, :] = jnp.sum(stt[8 * k:8 * k + 8] * q_t[None], axis=1)
    num = tbuf[0:64, :].T

    for p in range(2):
        q, kk, vv = proj[p].astype(F32), proj[2 + p].astype(F32) * 0.125, proj[4 + p].astype(F32)
        gate = proj[6 + p].astype(F32)
        h0, h1 = 2 * p, 2 * p + 1

        def two(v):
            return v[:, h0:h0 + 1], v[:, h1:h1 + 1]

        ko, kn = two(keep_old), two(keep_new)
        num0 = jnp.concatenate(
            [num[ROWS * h0:ROWS * (h0 + 1)], num[ROWS * h1:ROWS * (h1 + 1)]], axis=1
        )
        norm_in = jnp.concatenate([sn[:, h0, :], sn[:, h1, :]], axis=1)
        norm_new = spread(ko) * norm_in + spread(kn) * kk
        nnorm_ref[:, h0, :] = norm_new[:, 0:64]
        nnorm_ref[:, h1, :] = norm_new[:, 64:128]
        den = pair_sum(norm_new * q)
        kq = pair_sum(kk * q)
        fl = two(floor)
        bottom = tuple(jnp.maximum(jnp.abs(den[i]), fl[i]) for i in range(2))
        read = (spread(ko) * num0 + spread(kn) * vv * spread(kq)) / spread(bottom)
        mean = tuple(v * (1.0 / 64) for v in pair_sum(read))
        centered = read - spread(mean)
        var = tuple(v * (1.0 / 64) for v in pair_sum(centered * centered))
        scaled = centered * lax.rsqrt(spread(var) + 1e-06)
        at = slice(p * 128, (p + 1) * 128)
        cell[:, at] = (scaled * hg[:, at] * jax.nn.sigmoid(gate)).astype(BF16)

    arrived(wof.at[:, 0:15], one_r.at[6])
    for d in (1, 7, 3, 5, 4):
        zs = zpeer(d)
        if d == 4:
            arrived(wofb.at[zs, 0:8], e_r.at[zs])
            arrived(wofb.at[zs, 8:16], e4_r)
        else:
            arrived(wofb.at[zs], e_r.at[zs])
    p_my[...] = (
        nt_dot(cell[:, 0:128], wof[...].reshape(D, 128))
        + nt_dot(cell[:, 128:256], wofb[...].reshape(D, 128))
    ).astype(BF16)
    swap = push(p_my, p_ot, one_s.at[8], one_r.at[8], partner)
    swap.start()
    swap.wait_recv()
    both = p_my[...].astype(F32) + p_ot[...].astype(F32)
    rsd = (tok[...].astype(F32) + both).astype(BF16)
    resid[...] = rsd
    ntwo[...] = rms_scale(rsd.astype(F32), fgain[...]).astype(BF16)

    def cols(s, k):
        return pl.ds(pl.multiple_of(s * HALF + k * 128, 128), 128)

    xr = jnp.concatenate([ntwo[:, cols(c, k)] for k in range(8)], axis=0)

    def d_send(to, e):
        return push(outt.at[e], rcv.at[c, me], one_s.at[9], d_r.at[z], to)

    def plane256(zt):
        return pl.ds(pl.multiple_of(zt * 256, 256), 256)

    def plane16(zt):
        return pl.ds(zt * NP, NP)

    def dispatch(i, zt):
        rows = nn_dot(amat[plane256(zt), :], xr).astype(BF16)
        outt[plane16(zt)] = rows.reshape(NP, 16, 128)

    planes(dispatch)
    send_all(d_send)
    rcv[c, me] = outt[me]

    def write_one(b):
        for h in range(4):
            vth = vt[h // 2, 64 * (h % 2):64 * (h % 2 + 1), :]
            pick = jnp.where(
                lax.broadcasted_iota(jnp.int32, (64, ROWS), 1) == b, vth.astype(F32), 0.0
            ).astype(BF16)
            outer = nn_dot(pick, kcol[h])
            at = pl.ds(pl.multiple_of((b * 4 + h) * 64, 64), 64)
            nmat_ref[at, :] = keep[h, pl.ds(b, 1), :] * st[at, :] + scal[h, pl.ds(b, 1), :] * outer

    loop(0, ROWS, write_one)

    def h_view(s, zs):
        return rcv.at[s, plane16(zs)]

    def h_send(zs):
        return push(h_view(c, zs), h_view(c, zs), h_s, h_r.at[zs], partner)

    def unpack(s, zs):
        xf[...] = rcv[s, plane16(zs)].astype(F32).reshape(256, 128)
        at = pl.ds(pl.multiple_of(zs * ROWS, ROWS), ROWS)
        for k in range(8):
            xm[at, cols(s, k)] = xf[pl.ds(k, ROWS, stride=8), :].astype(BF16)

    for off in (*ZOFF, 0):
        zs = (z + NZ - off) % NZ
        if off:
            arrived(rcv.at[c, plane16(zs)], d_r.at[zs])
        else:
            arrived(rcv.at[c, 0:15], d_r.at[zs])
        h_send(zs).start()
        unpack(c, zs)
    for load in loads[18:]:
        load.wait()

    parts = ((0, 256), (256, 512), (512, DE))
    for lo, hi in parts:
        ga[:, lo:hi] = nt_dot(xm[:, half], eg[lo:hi, half])
        ua[:, lo:hi] = nt_dot(xm[:, half], eu[lo:hi, half])

    for off in (*ZOFF, 0):
        zs = (z + NZ - off) % NZ
        arrived(h_view(1 - c, zs), h_r.at[zs])
        unpack(1 - c, zs)

    for lo, hi in parts:
        gate = ga[:, lo:hi] + nt_dot(xm[:, other], eg[lo:hi, other])
        up = ua[:, lo:hi] + nt_dot(xm[:, other], eu[lo:hi, other])
        hid[:, lo:hi] = (gate * jax.nn.sigmoid(gate) * up).astype(BF16)

    def down(s, k):
        return nn_dot(hid[...], ed[:, pl.ds(pl.multiple_of(s * HALF + k * 256, 256), 256)]).astype(BF16)

    def k_send(k):
        return push(pd.at[k], pd_ot.at[k], one_s.at[10], k_r.at[k], partner)

    for k in range(4):
        pd[k] = down(1 - c, k)
        k_send(k).start()
    for k in range(4):
        own[k] = down(c, k)
    for k in range(4):
        arrived(pd_ot.at[k], k_r.at[k])
        both = own[k].astype(F32) + pd_ot[k].astype(F32)
        for h in range(2):
            yf[pl.ds(2 * k + h, 256, stride=8), :] = both[:, 128 * h:128 * (h + 1)]

    def b_send(to, s):
        return push(back.at[s], ret.at[me], one_s.at[11], b_r.at[z], to)

    def give_back(i, zt):
        back[plane16(zt)] = yf[plane256(zt), :].astype(BF16).reshape(NP, 16, 128)

    planes(give_back)
    send_all(b_send)
    ret[me] = back[me]

    weighted = jnp.zeros((512, 128), F32)
    for off in (*ZOFF, 0):
        zs = (z + NZ - off) % NZ
        if off:
            arrived(ret.at[plane16(zs)], b_r.at[zs])
        else:
            arrived(ret.at[0:15], b_r.at[zs])
        weighted = weighted + nn_dot(wmat[:, plane256(zs)], ret[plane16(zs)].reshape(256, 128))
    for k in range(8):
        mixed_ref[:, cols(c, k)] = (
            resid[:, cols(c, k)].astype(F32)
            + (weighted[ROWS * k:ROWS * (k + 1)] + weighted[256 + ROWS * k:256 + ROWS * (k + 1)])
        ).astype(BF16)
    last = push(mixed_ref.at[:, half], mixed_ref.at[:, half], one_s.at[12], one_r.at[12], partner)
    last.start()

    left(wst.at[0:7], one_s.at[0])
    left(gst.at[0:7], one_s.at[1])
    left(woz.at[0:7], one_s.at[2])
    left(nall.at[0:4, :, half], one_s.at[3])
    left(nall.at[0:2, :, half], one_s.at[13])
    left(nall.at[0:1, :, half], one_s.at[14])
    left(wfull.at[:, 0:15], one_s.at[4])
    left(gt.at[0:15], one_s.at[5])
    left(wof.at[:, 0:15], one_s.at[6])
    left(wofb.at[0, 0:15], one_s.at[15])
    left(wofb.at[0:4], one_s.at[16])
    left(wofb.at[0:2], one_s.at[17])
    left(wofb.at[0:1], one_s.at[18])
    left(res.at[0:7], one_s.at[7])
    left(p_my, one_s.at[8])
    left(outt.at[0:127], one_s.at[9])
    left(pd, one_s.at[10])
    left(back.at[0:127], one_s.at[11])
    left(nall.at[0:7, :, half], f_s)
    left(outt, h_s)
    arrived(mixed_ref.at[:, other], one_r.at[12])
    last.wait_send()


PIECES = 8


def store_kernel(*refs):
    n = len(OUTS)
    sems = refs[-1]
    step = ROWS * 256 // PIECES
    pairs = [(refs[1].at[k * step:(k + 1) * step], refs[n + 1].at[k * step:(k + 1) * step]) for k in range(PIECES)]
    pairs += [(refs[k], refs[n + k]) for k in (0, 2, 3)]
    moves = [pltpu.make_async_copy(a, b, sems.at[k]) for k, (a, b) in enumerate(pairs)]
    for move in moves:
        move.start()
    for move in moves:
        move.wait()


def stored(*arrays):
    n = len(OUTS)
    return pl.pallas_call(
        store_kernel,
        name="store",
        out_shape=tuple(jax.ShapeDtypeStruct(shape, kind) for shape, kind in OUTS),
        in_specs=[pl.BlockSpec(memory_space=pltpu.VMEM)] * n,
        out_specs=(pl.BlockSpec(memory_space=pl.ANY),) * n,
        scratch_shapes=[pltpu.SemaphoreType.DMA((n - 1 + PIECES,))],
        compiler_params=pltpu.CompilerParams(vmem_limit_bytes=8 << 20),
    )(*arrays)


def fused(*args):
    dma = pltpu.SemaphoreType.DMA
    vm = pl.BlockSpec(memory_space=pltpu.VMEM)
    hbm = pl.BlockSpec(memory_space=pltpu.HBM)

    def buf(shape, kind=BF16):
        return pltpu.VMEM(shape, kind)

    staged = [buf(a.shape if a.ndim < 3 or a.shape[0] != 1 else a.shape[1:], a.dtype) for a in args]
    return pl.pallas_call(
        fused_kernel,
        name="layer",
        out_shape=tuple(pltpu.VMEM(shape, kind) for shape, kind in OUTS),
        in_specs=[hbm] * len(args),
        out_specs=(vm, vm, vm, vm),
        scratch_shapes=[
            *staged,
            buf((64, 64, 128), F32),
            buf((NZ, ROWS, D)),
            buf((NZ, 16, 128)),
            buf((NZ, 16, 128)),
            buf((16, 128)),
            buf((16, 128)),
            buf((NZ, NP, 16, 128)),
            buf((NP, 16, 128)),
            buf((NZ, 16, 128)),
            buf((NZ, NP, 16, 128)),
            buf((NZ, NP, 16, 128)),
            buf((NZ, ROWS, 128)),
            buf((NZ, ROWS, 128)),
            buf((128, 128), F32),
            buf((8, 128), F32),
            buf((4, ROWS, 64), F32),
            buf((4, ROWS, 64)),
            buf((4, ROWS, 64), F32),
            buf((4, ROWS, 64), F32),
            buf((2, 128, ROWS)),
            buf((ROWS, 256)),
            buf((ROWS, D)),
            buf((ROWS, D)),
            buf((ROWS, D)),
            buf((ROWS, D)),
            buf((2048, 256)),
            buf((512, 2048)),
            buf((128, 16, 128)),
            buf((2, 128, 16, 128)),
            buf((256, 128), F32),
            buf((256, D)),
            buf((256, DE), F32),
            buf((256, DE), F32),
            buf((256, DE)),
            buf((4, 256, 256)),
            buf((4, 256, 256)),
            buf((4, 256, 256)),
            buf((2048, 128), F32),
            buf((128, 16, 128)),
            buf((128, 16, 128)),
            dma((len(args),)),
            dma((2, NZ)),
            dma((NZ,)),
            dma,
            dma,
            dma((NZ,)),
            dma((19,)),
            dma((19,)),
            dma((NZ,)),
            dma,
            dma((NZ,)),
            dma((4,)),
            dma((NZ,)),
        ],
        compiler_params=pltpu.CompilerParams(
            collective_id=0, has_side_effects=True, vmem_limit_bytes=40 << 20
        ),
    )(*(pltpu.with_memory_space_constraint(a, pltpu.HBM) for a in args))


def body(tokens, mix_gain, w_query, w_key, w_value, w_outgate, w_igate, w_fgate, igate_bias,
         fgate_bias, head_gain, w_out, state_matrix, state_norm, state_max, ffn_gain,
         w_expert_gate, w_expert_up, w_expert_down, routes, route_weights):
    mixed, new_matrix, new_norm, new_max = stored(*fused(
        tokens, mix_gain.reshape(1, D), w_query, w_key, w_value, w_outgate, w_igate.T, w_fgate.T,
        igate_bias.reshape(1, 4), fgate_bias.reshape(1, 4), head_gain.reshape(1, 256), w_out.T,
        state_max.T, state_norm, ffn_gain.reshape(1, D), routes.T, route_weights.T, state_matrix.reshape(ROWS * 256, 64),
        w_expert_gate.swapaxes(1, 2), w_expert_up.swapaxes(1, 2), w_expert_down,
    ))
    return (mixed, new_matrix.reshape(ROWS, 4, 64, 64), new_norm, new_max.T)


def solution(mesh):
    torus = Mesh(mesh.devices.reshape(NZ, NY, NX, mesh.shape["tp"]), (*EP, "tp"))
    placed = (
        P(EP, None), P(), P(EP, "tp"), P(EP, "tp"), P(EP, "tp"), P(EP, "tp"), P(EP, "tp"),
        P(EP, "tp"), P("tp"), P("tp"), P("tp"), P("tp", EP), P(EP, "tp", None, None),
        P(EP, "tp", None), P(EP, "tp"), P(), P(EP, None, "tp"), P(EP, None, "tp"),
        P(EP, "tp", None), P(EP, None), P(EP, None),
    )
    return jax.shard_map(
        body,
        mesh=torus,
        in_specs=placed,
        out_specs=(P(EP, None), P(EP, "tp", None, None), P(EP, "tp", None), P(EP, "tp")),
        check_vma=False,
    )
```
